32 devices in a mesh: grp: 2 (over y), sp: 4 (over z), tp: 4 (over x, core).
Axes of the slice: x: 2, y: 2, z: 4, core: 2. Of those that a mesh axis runs over, the one named last changes fastest.
Arguments:
- source: bfloat16 [4096, 2048], P(('grp', 'sp', 'tp')), parts along dimension 0, may hold values from -8 to 8
- target: bfloat16 [1024, 2048], P(('grp', 'sp', 'tp')), parts along dimension 0, may hold values from -8 to 8
- source_gain: float32 [2048], replicated, may hold values from 0.1 to 1.9
- attend_gain: float32 [2, 2048], replicated, may hold values from 0.1 to 1.9
- query_weight: bfloat16 [2, 2048, 2048], P(None, None, 'tp'), may hold values from -4 to 4
- key_weight: bfloat16 [2, 2048, 2048], P(None, None, 'tp'), may hold values from -4 to 4
- value_weight: bfloat16 [2, 2048, 2048], P(None, None, 'tp'), may hold values from -0.125 to 0.125
- out_weight: bfloat16 [2, 2048, 2048], P(None, 'tp'), may hold values from -3 to 3
- mixer_gain: float32 [2048], replicated, may hold values from 0.1 to 1.9
- gate_weight: bfloat16 [2048, 2816], P(None, 'tp'), may hold values from -0.125 to 0.125
- up_weight: bfloat16 [2048, 2816], P(None, 'tp'), may hold values from -0.125 to 0.125
- gate_taps: float32 [3, 2816], P(None, 'tp'), may hold values from -3 to 3
- up_taps: float32 [3, 2816], P(None, 'tp'), may hold values from -3 to 3
- down_weight: bfloat16 [2816, 2048], P('tp'), may hold values from -0.109375 to 0.109375
- final_gain: float32 [2048], replicated, may hold values from 0.1 to 1.9
Outputs:
- result: bfloat16 [1024, 2048], P(('grp', 'sp', 'tp')), parts along dimension 0
The draws below stay inside these ranges and needn't reach their ends.
There are 2 independent parts, one for each index of `grp`. The reference program is written for one: setup_inputs(seed, part) draws one part's arguments, and reference() takes and returns one part's arrays. A program takes and returns all parts, laid end to end along the dimension named above; an argument that names none is the same for every part. Nothing has to cross between parts.
All inputs are finite; a program needn't handle non-finite values.
Results may differ from the reference program's by a relative error of at most 0.04.
Values may be sent and summed in bfloat16 or wider, within the bound.
A program may use at most 128 MiB of HBM per device.

```python
import jax
import jax.numpy as jnp
from jax import lax

D = 2048
HEADS = 8
FF = 2816
HD = 256
SRC = 2048
TGT = 512


def projection_draw(key, salt_value):
    stacked = []
    for layer_number in range(2):
        base_draw = jax.random.normal(jax.random.fold_in(key, salt_value * 10 + layer_number), (D, D), jnp.float32)
        layer_matrix = jnp.clip(base_draw, -6.0, 6.0) * D ** (-0.5)
        stacked.append(jnp.clip(layer_matrix, -4.0, 4.0))
    return jnp.stack(stacked).astype(jnp.bfloat16)


def row_draw(key, row_count):
    base_rows = jnp.clip(jax.random.normal(jax.random.fold_in(key, 1), (row_count, D), jnp.float32), -6.0, 6.0)
    return base_rows.astype(jnp.bfloat16)


def draw_source(key, part):
    return row_draw(key, SRC)


def draw_target(key, part):
    return row_draw(key, TGT)


def draw_query_weight(key, part):
    return projection_draw(key, 1)


def draw_key_weight(key, part):
    return projection_draw(key, 2)


def steps_of(own_key, shape, pieces, low, largest):
    level = 1.0
    for position, shards_of in pieces:
        draws = jax.random.uniform(jax.random.fold_in(jax.random.fold_in(own_key, 6), position), (shards_of,), jnp.float32, low / len(pieces), largest / len(pieces))
        level = level * jnp.repeat(jnp.exp(draws), shape[position] // shards_of).reshape((-1,) + (1,) * (len(shape) - 1 - position))
    return level


def centred(rng, extent, width, limit, split=(), kind=jnp.bfloat16):
    level = steps_of(rng, extent, split, -0.22, 0.18) if split else 1.0
    entries = jax.random.normal(rng, extent, jnp.float32) * width * level
    return jnp.minimum(jnp.maximum(entries, -limit), limit).astype(kind)


def setup_inputs(seed: int = 0, part: int = 0) -> dict:
    keys = jax.random.split(jax.random.key(seed), 16)
    own_keys = jax.random.split(jax.random.fold_in(keys[15], part), 16)
    return {
        "source": draw_source(jax.random.fold_in(jax.random.fold_in(keys[15], part), 71), part),
        "target": draw_target(jax.random.fold_in(jax.random.fold_in(keys[15], part), 71), part),
        "source_gain": jnp.clip(1.0 + 0.18 * jax.random.normal(keys[2], (D,), jnp.float32), 0.1, 1.9),
        "attend_gain": jnp.clip(1.0 + 0.18 * jax.random.normal(keys[3], (2, D), jnp.float32), 0.1, 1.9),
        "query_weight": draw_query_weight(jax.random.fold_in(keys[15], 71), part),
        "key_weight": draw_key_weight(jax.random.fold_in(keys[15], 71), part),
        "value_weight": centred(keys[6], (2, D, D), D ** -0.5, 0.125, ((2, 4),)),
        "out_weight": centred(keys[7], (2, D, D), 4 ** -0.5, 3.0, ((1, 4),)),
        "mixer_gain": jnp.clip(1.0 + 0.18 * jax.random.normal(keys[8], (D,), jnp.float32), 0.1, 1.9),
        "gate_weight": centred(keys[9], (D, FF), D ** -0.5, 0.125, ((1, 4),)),
        "up_weight": centred(keys[10], (D, FF), D ** -0.5, 0.125, ((1, 4),)),
        "gate_taps": centred(keys[11], (3, FF), 0.6, 3.0, ((1, 4),), jnp.float32),
        "up_taps": centred(keys[12], (3, FF), 0.6, 3.0, ((1, 4),), jnp.float32),
        "down_weight": centred(keys[13], (FF, D), FF ** -0.5, 0.109375, ((0, 4),)),
        "final_gain": jnp.clip(1.0 + 0.18 * jax.random.normal(keys[14], (D,), jnp.float32), 0.1, 1.9),
    }


EPS = 1e-06

def normed_rows(rows, gain):
    wide = rows.astype(jnp.float32)
    return wide * lax.rsqrt(lax.optimization_barrier(jnp.mean(wide * wide, axis=-1, keepdims=True)) + EPS) * gain

def one_head(triple):
    query_head, key_head, value_head = triple
    scores = jnp.dot(query_head, key_head.T, preferred_element_type=jnp.float32) * HD ** (-0.5)
    highest = lax.optimization_barrier(jnp.max(scores, axis=-1, keepdims=True))
    raised = jnp.exp(scores - highest)
    totals = lax.optimization_barrier(jnp.sum(raised, axis=-1, keepdims=True))
    weights = raised.astype(jnp.bfloat16)
    summed = jnp.dot(weights, value_head, preferred_element_type=jnp.float32)
    return (summed / totals).astype(jnp.bfloat16)

def split_heads(block):
    return block.reshape(block.shape[0], HEADS, HD).transpose(1, 0, 2)

def reference(source, target, source_gain, attend_gain, query_weight, key_weight, value_weight, out_weight, mixer_gain, gate_weight, up_weight, gate_taps, up_taps, down_weight, final_gain):
    source_normed = normed_rows(source, source_gain).astype(jnp.bfloat16)
    residual = target.astype(jnp.float32)
    for layer_number in range(2):
        normed = normed_rows(residual, attend_gain[layer_number]).astype(jnp.bfloat16)
        query_block = jnp.dot(normed, query_weight[layer_number], preferred_element_type=jnp.float32).astype(jnp.bfloat16)
        key_rows = jnp.dot(source_normed, key_weight[layer_number], preferred_element_type=jnp.float32).astype(jnp.bfloat16)
        value_rows = jnp.dot(source_normed, value_weight[layer_number], preferred_element_type=jnp.float32).astype(jnp.bfloat16)
        attended = lax.map(one_head, (split_heads(query_block), split_heads(key_rows), split_heads(value_rows)))
        attended = attended.transpose(1, 0, 2).reshape(query_block.shape[0], D)
        residual = residual + jnp.dot(attended, out_weight[layer_number], preferred_element_type=jnp.float32)
    mixed = normed_rows(residual, mixer_gain).astype(jnp.bfloat16)
    gated = jnp.dot(mixed, gate_weight, preferred_element_type=jnp.float32).astype(jnp.bfloat16)
    upped = jnp.dot(mixed, up_weight, preferred_element_type=jnp.float32).astype(jnp.bfloat16)
    zero_rows = jnp.zeros((2, FF), jnp.float32)
    gate_pad = jnp.concatenate([zero_rows, gated.astype(jnp.float32)], axis=0)
    up_pad = jnp.concatenate([zero_rows, upped.astype(jnp.float32)], axis=0)
    gate_conv = gate_taps[0] * gate_pad[:-2] + gate_taps[1] * gate_pad[1:-1] + gate_taps[2] * gate_pad[2:]
    up_conv = up_taps[0] * up_pad[:-2] + up_taps[1] * up_pad[1:-1] + up_taps[2] * up_pad[2:]
    hidden = (jax.nn.silu(gate_conv) * up_conv).astype(jnp.bfloat16)
    residual = residual + jnp.dot(hidden, down_weight, preferred_element_type=jnp.float32)
    return normed_rows(residual, final_gain).astype(jnp.bfloat16)
```

```python
import functools

import jax
import jax.numpy as jnp
from jax import lax
from jax.experimental import pallas as pl
from jax.experimental.pallas import tpu as pltpu
from jax.sharding import PartitionSpec as P

HD = 256
EPS = 1e-06
STAT_ROWS = 8
LANES = 128
SOURCE_CHUNKS = 4
COLUMN_CHUNKS = 4
GROUP_ROWS = 256
MESH = pl.DeviceIdType.MESH
BF = jnp.bfloat16
F32 = jnp.float32


def normed_rows(wide, gain):
    return wide * lax.rsqrt(jnp.mean(wide * wide, axis=-1, keepdims=True) + EPS) * gain


def mm(a, b):
    return jnp.dot(a, b, preferred_element_type=F32)


def scope(name):
    return jax.named_scope(name)


def kernel(
    n,
    S,
    source,
    target,
    source_gain_in,
    attend_gain_in,
    query_weight,
    key_weight,
    value_weight,
    out_weight,
    mixer_gain_in,
    gate_weight,
    up_weight,
    gate_taps_in,
    up_taps_in,
    down_weight,
    final_gain_in,
    result,
    source_gain,
    attend_gain,
    mixer_gain,
    final_gain,
    gate_taps,
    up_taps,
    sv,
    traw,
    wq,
    wkv,
    wo,
    wg,
    wu,
    wd,
    xs,
    xt,
    kv,
    qall,
    osend,
    orecv,
    ssend,
    srecv,
    pf,
    att,
    p1s,
    p1r,
    p2s,
    p2r,
    dpf,
    d1s,
    d1r,
    d2s,
    d2r,
    hs,
    hr,
    gpad,
    upad,
    hid,
    residual,
    out_rows,
    load_sem,
    tr_send,
    tr_recv,
    n_send,
    n_recv,
    sx_send,
    sx_recv,
    sd_send,
    sd_recv,
    q_send,
    q_recv,
    r_send,
    r_recv,
    s_send,
    s_recv,
    p1_send,
    p1_recv,
    p2_send,
    p2_recv,
    d1_send,
    d1_recv,
    d2_send,
    d2_recv,
    h_send,
    h_recv,
):
    X = n // 2
    Rs, D = source.shape
    Rt = target.shape[0]
    W = wq.shape[2]
    H = 2 * Rt
    T = n * Rt
    heads = W // HD
    F = wg.shape[0]
    NC = xs.shape[1]
    RC = Rs // NC
    C = p1s.shape[2]
    DC = D // C
    scale = HD ** (-0.5)
    t = lax.axis_index("tp")
    s = lax.axis_index("sp")
    x = lax.div(t, 2)
    c = lax.rem(t, 2)
    other = 1 - c
    peer = x * 2 + other
    pending = []

    def chip_at(k):
        return lax.rem(x + k, X)

    def remote(src, dst, ss, rs, axis, where):
        return pltpu.make_async_remote_copy(
            src_ref=src,
            dst_ref=dst,
            send_sem=ss,
            recv_sem=rs,
            device_id={axis: where},
            device_id_type=MESH,
        )

    def launch(copy):
        copy.start()
        pending.append(copy)

    far_blocks = []
    low = s * 0
    high = low + (S - 1)
    for _ in range(S - 1):
        left = lax.div(2 * s - low - high + S, S)
        far_blocks.append(left * low + (1 - left) * high)
        low = low + left
        high = high - (1 - left)

    barrier = pltpu.get_barrier_semaphore()
    pl.semaphore_signal(barrier, inc=1, device_id={"tp": peer}, device_id_type=MESH)
    for k in range(1, X):
        pl.semaphore_signal(
            barrier, inc=1, device_id={"tp": chip_at(k) * 2 + c}, device_id_type=MESH
        )
    for block in far_blocks:
        pl.semaphore_signal(barrier, inc=1, device_id={"sp": block}, device_id_type=MESH)

    loads = iter(range(22))

    def load(src, dst):
        return pltpu.make_async_copy(src, dst, load_sem.at[next(loads)])

    load_t = load(target, traw.at[x])
    load_s = load(source, sv)
    load_small = [
        load(attend_gain_in, attend_gain),
        load(source_gain_in, source_gain),
    ]
    load_late = [
        load(mixer_gain_in, mixer_gain),
        load(final_gain_in, final_gain),
        load(gate_taps_in, gate_taps),
        load(up_taps_in, up_taps),
    ]
    load_q = [load(query_weight.at[l], wq.at[l]) for l in range(2)]
    load_kv = [
        [load(key_weight.at[l], wkv.at[2 * l]), load(value_weight.at[l], wkv.at[2 * l + 1])]
        for l in range(2)
    ]
    load_o = [load(out_weight.at[l], wo.at[l]) for l in range(2)]
    load_m = [load(gate_weight, wg), load(up_weight, wu), load(down_weight, wd)]
    for copy in [load_t, *load_small, load_s, load_q[0]]:
        copy.start()

    def target_copy(k, where):
        return remote(traw.at[k], traw.at[k], tr_send.at[where], tr_recv.at[k], "tp", where * 2 + c)

    def normed_copy(a, k, core):
        return remote(xt.at[a, k, core], xt.at[a, k, core], n_send.at[a, k], n_recv.at[a, k], "tp", peer)

    def source_copy(ch, k, where):
        return remote(
            xs.at[k, ch, c], xs.at[k, ch, c], sx_send.at[ch, where], sx_recv.at[ch, k], "tp", where * 2 + c
        )

    def source_peer(ch, k, core):
        return remote(
            xs.at[k, ch, core], xs.at[k, ch, core], sd_send.at[ch, k], sd_recv.at[ch, k], "tp", peer
        )

    def share_rows(a, k, gain):
        xt[a, k, c] = normed_rows(residual[k], gain).astype(BF)
        launch(normed_copy(a, k, c))

    def shared_rows(a, k):
        normed_copy(a, k, other).wait_recv()
        return xt[a, k].reshape(H, D)

    def query_copy(layer, k, j, block, where):
        return remote(
            qall.at[layer, k, block],
            qall.at[layer, k, block],
            q_send.at[layer, k, j],
            q_recv.at[layer, k, block],
            "sp",
            where,
        )

    def send_queries(layer, k):
        qall[layer, k, s] = mm(shared_rows(layer, k), wq[layer]).astype(BF)
        for j, block in enumerate(far_blocks):
            launch(query_copy(layer, k, j, s, block))

    def project_chip(layer):
        rows = xs[x].reshape(2 * Rs, D)

        def one(j, carry):
            kv[j, x] = mm(rows, wkv[j]).astype(BF).reshape(NC, 2 * RC, W)
            return carry

        lax.fori_loop(2 * layer, 2 * layer + 2, one, 0)

    def project_chunk(low, high, k, ch):
        rows = xs[k, ch].reshape(2 * RC, D)

        def one(j, carry):
            kv[j, k, ch] = mm(rows, wkv[j]).astype(BF)
            return carry

        lax.fori_loop(low, high, one, 0)

    def sums_copy(layer, k, j, slot, block):
        return remote(
            osend.at[layer, k, block],
            orecv.at[layer, k, slot],
            r_send.at[layer, k, j],
            r_recv.at[layer, k, slot],
            "sp",
            block,
        )

    def stats_copy(layer, k, j, slot, block):
        return remote(
            ssend.at[layer, k, block],
            srecv.at[layer, k, slot],
            s_send.at[layer, k, j],
            s_recv.at[layer, k, slot],
            "sp",
            block,
        )

    G = max(1, min(S, GROUP_ROWS // H))
    while S % G:
        G -= 1

    def attend(layer, k):
        for j, block in enumerate(far_blocks):
            query_copy(layer, k, j, block, block).wait_recv()

        def group(base):
            blocks = pl.ds(base, G)
            lanes = lax.broadcasted_iota(jnp.int32, (G * H, LANES), 1)
            packed = jnp.zeros((G * H, LANES), F32)
            for h in range(heads):
                cols = slice(h * HD, (h + 1) * HD)
                query = qall[layer, k, blocks, :, cols].reshape(G * H, HD)
                keys = kv[2 * layer, :, :, :, cols].reshape(n * Rs, HD)
                values = kv[2 * layer + 1, :, :, :, cols].reshape(n * Rs, HD)
                scores = (
                    lax.dot_general(
                        query, keys, (((1,), (1,)), ((), ())), preferred_element_type=F32
                    )
                    * scale
                )
                top = jnp.max(scores, axis=-1, keepdims=True)
                raised = jnp.exp(scores - top)
                total = jnp.sum(raised, axis=-1, keepdims=True)
                osend[layer, k, blocks, :, cols] = (
                    mm(raised.astype(BF), values).astype(BF).reshape(G, H, HD)
                )
                packed = jnp.where(lanes == 2 * h, top, packed)
                packed = jnp.where(lanes == 2 * h + 1, total, packed)
            stats = packed.T[:STAT_ROWS]
            for b in range(G):
                ssend[layer, k, base + b] = stats[:, b * H : (b + 1) * H]

        if G == S:
            group(0)
        else:

            def one(g, carry):
                group(g * G)
                return carry

            lax.fori_loop(0, S // G, one, 0)
        for j, block in enumerate(far_blocks):
            launch(stats_copy(layer, k, j, s, block))
            launch(sums_copy(layer, k, j, s, block))
        orecv[layer, k, s] = osend[layer, k, s]
        srecv[layer, k, s] = ssend[layer, k, s]

    def pair_copy(layer, k, ch):
        return remote(
            p1s.at[layer, k, ch],
            p1r.at[layer, k, ch],
            p1_send.at[layer, k, ch],
            p1_recv.at[layer, k, ch],
            "tp",
            peer,
        )

    def chip_copy(layer, k, ch, slot, where):
        return remote(
            p2s.at[layer, k, ch],
            p2r.at[layer, k, ch, slot],
            p2_send.at[layer, k, ch, where],
            p2_recv.at[layer, k, ch, slot],
            "tp",
            where * 2 + c,
        )

    def combine(layer, k):
        for j, block in enumerate(far_blocks):
            stats_copy(layer, k, j, block, block).wait_recv()
            sums_copy(layer, k, j, block, block).wait_recv()
        rows = srecv[layer, k].reshape(S * STAT_ROWS, H)
        if S * STAT_ROWS < LANES:
            rows = jnp.concatenate([rows, jnp.zeros((LANES - S * STAT_ROWS, H), F32)], axis=0)
        stats = rows.T
        for h in range(heads):
            cols = slice(h * HD, (h + 1) * HD)
            tops = [stats[:, b * STAT_ROWS + 2 * h :][:, :1] for b in range(S)]
            highest = functools.reduce(jnp.maximum, tops)
            total = jnp.zeros((H, 1), F32)
            summed = jnp.zeros((H, HD), F32)
            for b in range(S):
                factor = jnp.exp(tops[b] - highest)
                total = total + factor * stats[:, b * STAT_ROWS + 2 * h + 1 :][:, :1]
                summed = summed + factor * orecv[layer, k, b, :, cols].astype(F32)
            att[k, :, cols] = (summed / total).astype(BF)
        rows = att[k]
        for ch in range(C):
            cols = slice(ch * DC, (ch + 1) * DC)
            pf[k, :, :, cols] = mm(rows, wo[layer, :, cols]).reshape(2, Rt, DC)
            p1s[layer, k, ch] = pf[k, other, :, cols].astype(BF)
            launch(pair_copy(layer, k, ch))

    def spread(layer, k):
        for ch in range(C):
            cols = slice(ch * DC, (ch + 1) * DC)
            pair_copy(layer, k, ch).wait_recv()
            chip_sum = pf[k, c, :, cols] + p1r[layer, k, ch].astype(F32)
            p2s[layer, k, ch] = chip_sum.astype(BF)
            for i in range(1, X):
                launch(chip_copy(layer, k, ch, x, chip_at(i)))
            residual[k, :, cols] = residual[k, :, cols] + chip_sum

    def settle(layer, k, gain):
        for ch in range(C):
            cols = slice(ch * DC, (ch + 1) * DC)
            for i in range(1, X):
                chip_copy(layer, k, ch, chip_at(i), chip_at(i)).wait_recv()
                residual[k, :, cols] = residual[k, :, cols] + p2r[
                    layer, k, ch, chip_at(i)
                ].astype(F32)
        share_rows(layer + 1, k, gain)

    def finish_read(layer, gain, follow):
        for k in range(X):
            with scope(f"combine{layer}{k}"):
                combine(layer, k)
            if k:
                with scope(f"settle{layer}{k - 1}"):
                    settle(layer, k - 1, gain)
            with scope(f"spread{layer}{k}"):
                spread(layer, k)
            if k:
                with scope(f"follow{layer}{k - 1}"):
                    follow(k - 1)
        with scope(f"settle{layer}{X - 1}"):
            settle(layer, X - 1, gain)
        with scope(f"follow{layer}{X - 1}"):
            follow(X - 1)

    load_t.wait()
    with scope("barrier"):
        pl.semaphore_wait(barrier, X + S - 1)
    for i in range(1, X):
        launch(target_copy(x, chip_at(i)))
    for copy in load_kv[0]:
        copy.start()
    for copy in load_small:
        copy.wait()
    residual[x] = traw[x].astype(F32)
    share_rows(0, x, attend_gain[0:1])
    load_s.wait()
    with scope("norm_source"):
        for ch in range(NC):
            rows = sv[ch * RC : (ch + 1) * RC].astype(F32)
            xs[x, ch, c] = normed_rows(rows, source_gain[...]).astype(BF)
            for i in range(1, X):
                launch(source_copy(ch, x, chip_at(i)))
            launch(source_peer(ch, x, c))
    with scope("q0own"):
        load_q[0].wait()
        send_queries(0, x)
    for copy in load_kv[1]:
        copy.start()
    with scope("proj_chip0"):
        for ch in range(NC):
            source_peer(ch, x, other).wait_recv()
        for copy in load_kv[0]:
            copy.wait()
        project_chip(0)
    with scope("target_far"):
        for i in range(1, X):
            k = chip_at(i)
            target_copy(k, k).wait_recv()
            residual[k] = traw[k].astype(F32)
            share_rows(0, k, attend_gain[0:1])
    for copy in [load_q[1], *load_o]:
        copy.start()
    with scope("proj_chip1"):
        for copy in load_kv[1]:
            copy.wait()
        project_chip(1)
    with scope("q0far"):
        for i in range(1, X):
            send_queries(0, chip_at(i))
    for copy in [*load_late, *load_m]:
        copy.start()
    for ch in range(NC):
        with scope(f"forward{ch}"):
            for i in range(1, X):
                k = chip_at(i)
                source_copy(ch, k, k).wait_recv()
                launch(source_peer(ch, k, c))
        if ch:
            with scope(f"proj{ch - 1}"):
                for i in range(1, X):
                    source_peer(ch - 1, chip_at(i), other).wait_recv()
                    project_chunk(0, 4, chip_at(i), ch - 1)
    with scope("proj_last"):
        for i in range(1, X):
            source_peer(NC - 1, chip_at(i), other).wait_recv()
            project_chunk(0, 2, chip_at(i), NC - 1)
    for k in range(X):
        with scope(f"attend0{k}"):
            attend(0, k)
    with scope("proj_rest"):
        for i in range(1, X):
            project_chunk(2, 4, chip_at(i), NC - 1)
    for copy in [*load_o, load_q[1]]:
        copy.wait()
    finish_read(0, attend_gain[1:2], lambda k: send_queries(1, k))
    for k in range(X):
        with scope(f"attend1{k}"):
            attend(1, k)
    for copy in [*load_late, *load_m]:
        copy.wait()
    pads = ((gpad, wg), (upad, wu))

    def halo_out(number):
        return remote(
            hs.at[number],
            hr.at[number],
            h_send.at[number],
            h_recv.at[number],
            "sp",
            lax.rem(s + 1, S),
        )

    def lift(k):
        mixed = shared_rows(2, k)
        for number, (pad, weight) in enumerate(pads):
            lifted = (
                lax.dot_general(
                    mixed, weight[...], (((1,), (1,)), ((), ())), preferred_element_type=F32
                )
                .astype(BF)
                .astype(F32)
            )
            if k == X - 1:
                hs[number] = lifted[H - 8 :]

                @pl.when(s < S - 1)
                def _():
                    halo_out(number).start()

            pad[8 + k * H : 8 + (k + 1) * H] = lifted

    finish_read(1, mixer_gain[...], lift)

    def hidden_rows(start, stop):
        def convolved(pad, taps):
            return (
                taps[0:1] * pad[6 + start : 6 + stop]
                + taps[1:2] * pad[7 + start : 7 + stop]
                + taps[2:3] * pad[8 + start : 8 + stop]
            )

        gate = convolved(gpad, gate_taps)
        hid[start:stop] = (gate / (1.0 + jnp.exp(-gate)) * convolved(upad, up_taps)).astype(BF)

    with scope("hidden"):
        hidden_rows(16, T)

    @pl.when(s == 0)
    def _():
        for pad, _weight in pads:
            pad[:8] = jnp.zeros((8, F), F32)

    @pl.when(s > 0)
    def _():
        for number, (pad, _weight) in enumerate(pads):
            halo_out(number).wait_recv()
            pad[:8] = hr[number]

    @pl.when(s < S - 1)
    def _():
        for number in range(2):
            halo_out(number).wait_send()

    hidden_rows(0, 16)

    def down_pair(ch):
        return remote(d1s.at[ch], d1r.at[ch], d1_send.at[ch], d1_recv.at[ch], "tp", peer)

    def down_chip(ch, i, slot, where):
        return remote(
            d2s.at[ch, i],
            d2r.at[ch, slot],
            d2_send.at[ch, i],
            d2_recv.at[ch, slot],
            "tp",
            where * 2 + c,
        )

    with scope("down_mm"):
        rows = hid[...]
        for ch in range(C):
            cols = slice(ch * DC, (ch + 1) * DC)
            dpf[:, :, :, cols] = mm(rows, wd[:, cols]).reshape(X, 2, Rt, DC)
            d1s[ch] = dpf[:, other, :, cols].astype(BF)
            launch(down_pair(ch))
    with scope("down_pair"):
        for ch in range(C):
            cols = slice(ch * DC, (ch + 1) * DC)
            down_pair(ch).wait_recv()
            for i in range(1, X):
                k = chip_at(i)
                d2s[ch, i] = (dpf[k, c, :, cols] + d1r[ch, k].astype(F32)).astype(BF)
                launch(down_chip(ch, i, x, k))
            residual[x, :, cols] = (
                residual[x, :, cols] + dpf[x, c, :, cols] + d1r[ch, x].astype(F32)
            )
    with scope("down_far"):
        for ch in range(C):
            cols = slice(ch * DC, (ch + 1) * DC)
            for i in range(1, X):
                k = chip_at(i)
                down_chip(ch, i, k, k).wait_recv()
                residual[x, :, cols] = residual[x, :, cols] + d2r[ch, k].astype(F32)
    out_rows[...] = normed_rows(residual[x], final_gain[...]).astype(BF)
    write = load(out_rows, result)
    write.start()
    for copy in pending:
        copy.wait_send()
    write.wait()


def body(n, S, *arrays):
    (
        source,
        target,
        source_gain,
        attend_gain,
        query_weight,
        key_weight,
        value_weight,
        out_weight,
        mixer_gain,
        gate_weight,
        up_weight,
        gate_taps,
        up_taps,
        down_weight,
        final_gain,
    ) = arrays
    Rs, D = source.shape
    Rt = target.shape[0]
    W = query_weight.shape[2]
    F = gate_weight.shape[1]
    T = n * Rt
    H = 2 * Rt
    X = n // 2
    NC = SOURCE_CHUNKS
    C = COLUMN_CHUNKS
    RC = Rs // NC
    DC = D // C
    hbm = pl.BlockSpec(memory_space=pl.ANY)
    dma = pltpu.SemaphoreType.DMA
    scratch = [
        pltpu.VMEM((1, D), F32),
        pltpu.VMEM((2, D), F32),
        pltpu.VMEM((1, D), F32),
        pltpu.VMEM((1, D), F32),
        pltpu.VMEM((3, F), F32),
        pltpu.VMEM((3, F), F32),
        pltpu.VMEM((Rs, D), BF),
        pltpu.VMEM((X, Rt, D), BF),
        pltpu.VMEM((2, D, W), BF),
        pltpu.VMEM((4, D, W), BF),
        pltpu.VMEM((2, W, D), BF),
        pltpu.VMEM((F, D), BF),
        pltpu.VMEM((F, D), BF),
        pltpu.VMEM((F, D), BF),
        pltpu.VMEM((X, NC, 2, RC, D), BF),
        pltpu.VMEM((3, X, 2, Rt, D), BF),
        pltpu.VMEM((4, X, NC, 2 * RC, W), BF),
        pltpu.VMEM((2, X, S, H, W), BF),
        pltpu.VMEM((2, X, S, H, W), BF),
        pltpu.VMEM((2, X, S, H, W), BF),
        pltpu.VMEM((2, X, S, STAT_ROWS, H), F32),
        pltpu.VMEM((2, X, S, STAT_ROWS, H), F32),
        pltpu.VMEM((X, 2, Rt, D), F32),
        pltpu.VMEM((X, H, W), BF),
        pltpu.VMEM((2, X, C, Rt, DC), BF),
        pltpu.VMEM((2, X, C, Rt, DC), BF),
        pltpu.VMEM((2, X, C, Rt, DC), BF),
        pltpu.VMEM((2, X, C, X, Rt, DC), BF),
        pltpu.VMEM((X, 2, Rt, D), F32),
        pltpu.VMEM((C, X, Rt, DC), BF),
        pltpu.VMEM((C, X, Rt, DC), BF),
        pltpu.VMEM((C, X, Rt, DC), BF),
        pltpu.VMEM((C, X, Rt, DC), BF),
        pltpu.VMEM((2, 8, F), F32),
        pltpu.VMEM((2, 8, F), F32),
        pltpu.VMEM((T + 8, F), F32),
        pltpu.VMEM((T + 8, F), F32),
        pltpu.VMEM((T, F), BF),
        pltpu.VMEM((X, Rt, D), F32),
        pltpu.VMEM((Rt, D), BF),
        dma((22,)),
        dma((X,)),
        dma((X,)),
        dma((3, X)),
        dma((3, X)),
        dma((NC, X)),
        dma((NC, X)),
        dma((NC, X)),
        dma((NC, X)),
        dma((2, X, S)),
        dma((2, X, S)),
        dma((2, X, S)),
        dma((2, X, S)),
        dma((2, X, S)),
        dma((2, X, S)),
        dma((2, X, C)),
        dma((2, X, C)),
        dma((2, X, C, X)),
        dma((2, X, C, X)),
        dma((C,)),
        dma((C,)),
        dma((C, X)),
        dma((C, X)),
        dma((2,)),
        dma((2,)),
    ]
    return pl.pallas_call(
        functools.partial(kernel, n, S),
        out_shape=jax.ShapeDtypeStruct((Rt, D), BF),
        in_specs=[hbm] * 15,
        out_specs=hbm,
        scratch_shapes=scratch,
        compiler_params=pltpu.CompilerParams(
            collective_id=0, has_side_effects=True, vmem_limit_bytes=67043328
        ),
    )(
        source,
        target,
        source_gain.reshape(1, D),
        attend_gain,
        query_weight,
        key_weight,
        value_weight,
        out_weight,
        mixer_gain.reshape(1, D),
        gate_weight.T,
        up_weight.T,
        gate_taps,
        up_taps,
        down_weight,
        final_gain.reshape(1, D),
    )


def solution(mesh):
    placed = (
        P(("grp", "sp", "tp"), None),
        P(("grp", "sp", "tp"), None),
        P(),
        P(),
        P(None, None, "tp"),
        P(None, None, "tp"),
        P(None, None, "tp"),
        P(None, "tp", None),
        P(),
        P(None, "tp"),
        P(None, "tp"),
        P(None, "tp"),
        P(None, "tp"),
        P("tp", None),
        P(),
    )
    return jax.shard_map(
        functools.partial(body, mesh.shape["tp"], mesh.shape["sp"]),
        mesh=mesh,
        in_specs=placed,
        out_specs=P(("grp", "sp", "tp"), None),
        check_vma=False,
    )
```

```python
import functools

import jax
import jax.numpy as jnp
from jax import lax
from jax.experimental import pallas as pl
from jax.experimental.pallas import tpu as pltpu
from jax.sharding import PartitionSpec as P

HD = 256
EPS = 1e-06
STAT_ROWS = 8
LANES = 128
SOURCE_CHUNKS = 4
COLUMN_CHUNKS = 4
GROUP_ROWS = 256
MESH = pl.DeviceIdType.MESH
BF = jnp.bfloat16
F32 = jnp.float32


def normed_rows(wide, gain):
    return wide * lax.rsqrt(jnp.mean(wide * wide, axis=-1, keepdims=True) + EPS) * gain


def mm(a, b):
    return jnp.dot(a, b, preferred_element_type=F32)


def scope(name):
    return jax.named_scope(name)


def kernel(
    n,
    S,
    source,
    target,
    source_gain_in,
    attend_gain_in,
    query_weight,
    key_weight,
    value_weight,
    out_weight,
    mixer_gain_in,
    gate_weight,
    up_weight,
    gate_taps_in,
    up_taps_in,
    down_weight,
    final_gain_in,
    result,
    source_gain,
    attend_gain,
    mixer_gain,
    final_gain,
    gate_taps,
    up_taps,
    sv,
    traw,
    wq,
    wkv,
    wo,
    wg,
    wu,
    wgt,
    wut,
    wd,
    xs,
    xt,
    kv,
    qall,
    osend,
    orecv,
    ssend,
    srecv,
    pf,
    att,
    p1s,
    p1r,
    p2s,
    p2r,
    dpf,
    d1s,
    d1r,
    d2s,
    d2r,
    hs,
    hr,
    gpad,
    upad,
    hid,
    residual,
    load_sem,
    tr_send,
    tr_recv,
    n_send,
    n_recv,
    sx_send,
    sx_recv,
    sd_send,
    sd_recv,
    q_send,
    q_recv,
    r_send,
    r_recv,
    s_send,
    s_recv,
    p1_send,
    p1_recv,
    p2_send,
    p2_recv,
    d1_send,
    d1_recv,
    d2_send,
    d2_recv,
    h_send,
    h_recv,
):
    X = n // 2
    Rs, D = source.shape
    Rt = target.shape[0]
    W = wq.shape[2]
    H = 2 * Rt
    T = n * Rt
    heads = W // HD
    F = wg.shape[0]
    NC = xs.shape[1]
    RC = Rs // NC
    C = p1s.shape[2]
    DC = D // C
    scale = HD ** (-0.5)
    t = lax.axis_index("tp")
    s = lax.axis_index("sp")
    x = lax.div(t, 2)
    c = lax.rem(t, 2)
    other = 1 - c
    peer = x * 2 + other
    pending = []
    order = [*reversed(range(X))]

    def chip_at(k):
        return lax.rem(x + k, X)

    def remote(src, dst, ss, rs, axis, where):
        return pltpu.make_async_remote_copy(
            src_ref=src,
            dst_ref=dst,
            send_sem=ss,
            recv_sem=rs,
            device_id={axis: where},
            device_id_type=MESH,
        )

    def drain():
        while pending:
            pending.pop().wait_send()

    def launch(copy):
        copy.start()
        pending.append(copy)

    far_blocks = []
    low = s * 0
    high = low + (S - 1)
    for _ in range(S - 1):
        left = lax.div(2 * s - low - high + S, S)
        far_blocks.append(left * low + (1 - left) * high)
        low = low + left
        high = high - (1 - left)

    barrier = pltpu.get_barrier_semaphore()
    pl.semaphore_signal(barrier, inc=1, device_id={"tp": peer}, device_id_type=MESH)
    for k in range(1, X):
        pl.semaphore_signal(
            barrier, inc=1, device_id={"tp": chip_at(k) * 2 + c}, device_id_type=MESH
        )
    for block in far_blocks:
        pl.semaphore_signal(barrier, inc=1, device_id={"sp": block}, device_id_type=MESH)

    loads = iter(range(22))

    def load(src, dst):
        return pltpu.make_async_copy(src, dst, load_sem.at[next(loads)])

    load_t = load(target, traw.at[x])
    load_s = load(source, sv)
    load_small = [
        load(attend_gain_in, attend_gain),
        load(source_gain_in, source_gain),
    ]
    load_late = [
        load(mixer_gain_in, mixer_gain),
        load(final_gain_in, final_gain),
        load(gate_taps_in, gate_taps),
        load(up_taps_in, up_taps),
    ]
    load_q = [load(query_weight.at[l], wq.at[l]) for l in range(2)]
    load_kv = [
        [load(key_weight.at[l], wkv.at[2 * l]), load(value_weight.at[l], wkv.at[2 * l + 1])]
        for l in range(2)
    ]
    load_o = [load(out_weight.at[l], wo.at[l]) for l in range(2)]
    load_m = [load(gate_weight, wg), load(up_weight, wu), load(down_weight, wd)]
    for copy in [load_t, *load_small, load_s, load_q[0]]:
        copy.start()

    def target_copy(k, where):
        return remote(traw.at[k], traw.at[k], tr_send.at[where], tr_recv.at[k], "tp", where * 2 + c)

    def normed_copy(a, k, core):
        return remote(xt.at[a, k, core], xt.at[a, k, core], n_send.at[a, k], n_recv.at[a, k], "tp", peer)

    def source_copy(ch, k, where):
        return remote(
            xs.at[k, ch, c], xs.at[k, ch, c], sx_send.at[ch, where], sx_recv.at[ch, k], "tp", where * 2 + c
        )

    def source_peer(ch, k, core):
        return remote(
            xs.at[k, ch, core], xs.at[k, ch, core], sd_send.at[ch, k], sd_recv.at[ch, k], "tp", peer
        )

    def share_rows(a, k, gain):
        xt[a, k, c] = normed_rows(residual[k], gain).astype(BF)
        launch(normed_copy(a, k, c))

    def shared_rows(a, k):
        normed_copy(a, k, other).wait_recv()
        return xt[a, k].reshape(H, D)

    def query_copy(layer, k, j, block, where):
        return remote(
            qall.at[layer, k, block],
            qall.at[layer, k, block],
            q_send.at[layer, k, j],
            q_recv.at[layer, k, block],
            "sp",
            where,
        )

    def send_queries(layer, k):
        qall[layer, k, s] = mm(shared_rows(layer, k), wq[layer]).astype(BF)
        for j, block in enumerate(far_blocks):
            launch(query_copy(layer, k, j, s, block))

    def project_chip(layer, k):
        rows = xs[k].reshape(2 * Rs, D)

        def one(j, carry):
            kv[j, k] = mm(rows, wkv[j]).astype(BF).reshape(NC, 2 * RC, W)
            return carry

        lax.fori_loop(2 * layer, 2 * layer + 2, one, 0)

    def project_chunk(k, ch):
        rows = xs[k, ch].reshape(2 * RC, D)

        def one(j, carry):
            kv[j, k, ch] = mm(rows, wkv[j]).astype(BF)
            return carry

        lax.fori_loop(0, 2, one, 0)

    def sums_copy(layer, k, j, slot, block):
        return remote(
            osend.at[layer, k, block],
            orecv.at[layer, k, slot],
            r_send.at[layer, k, j],
            r_recv.at[layer, k, slot],
            "sp",
            block,
        )

    def stats_copy(layer, k, j, slot, block):
        return remote(
            ssend.at[layer, k, block],
            srecv.at[layer, k, slot],
            s_send.at[layer, k, j],
            s_recv.at[layer, k, slot],
            "sp",
            block,
        )

    G = max(1, min(S, GROUP_ROWS // H))
    while S % G:
        G -= 1

    def attend(layer, k):
        for j, block in enumerate(far_blocks):
            query_copy(layer, k, j, block, block).wait_recv()

        def group(base):
            blocks = pl.ds(base, G)
            lanes = lax.broadcasted_iota(jnp.int32, (G * H, LANES), 1)
            packed = jnp.zeros((G * H, LANES), F32)
            for h in range(heads):
                cols = slice(h * HD, (h + 1) * HD)
                query = qall[layer, k, blocks, :, cols].reshape(G * H, HD)
                keys = kv[2 * layer, :, :, :, cols].reshape(n * Rs, HD)
                values = kv[2 * layer + 1, :, :, :, cols].reshape(n * Rs, HD)
                scores = (
                    lax.dot_general(
                        query, keys, (((1,), (1,)), ((), ())), preferred_element_type=F32
                    )
                    * scale
                )
                top = jnp.max(scores, axis=-1, keepdims=True)
                raised = jnp.exp(scores - top)
                total = jnp.sum(raised, axis=-1, keepdims=True)
                osend[layer, k, blocks, :, cols] = (
                    mm(raised.astype(BF), values).astype(BF).reshape(G, H, HD)
                )
                packed = jnp.where(lanes == 2 * h, top, packed)
                packed = jnp.where(lanes == 2 * h + 1, total, packed)
            stats = packed.T[:STAT_ROWS]
            for b in range(G):
                ssend[layer, k, base + b] = stats[:, b * H : (b + 1) * H]

        if G == S:
            group(0)
        else:

            def one(g, carry):
                group(g * G)
                return carry

            lax.fori_loop(0, S // G, one, 0)
        for j, block in enumerate(far_blocks):
            launch(stats_copy(layer, k, j, s, block))
            launch(sums_copy(layer, k, j, s, block))
        orecv[layer, k, s] = osend[layer, k, s]
        srecv[layer, k, s] = ssend[layer, k, s]

    def pair_copy(layer, k, ch):
        return remote(
            p1s.at[layer, k, ch],
            p1r.at[layer, k, ch],
            p1_send.at[layer, k, ch],
            p1_recv.at[layer, k, ch],
            "tp",
            peer,
        )

    def chip_copy(layer, k, ch, slot, where):
        return remote(
            p2s.at[layer, k, ch],
            p2r.at[layer, k, ch, slot],
            p2_send.at[layer, k, ch, where],
            p2_recv.at[layer, k, ch, slot],
            "tp",
            where * 2 + c,
        )

    def combine(layer, k):
        for j, block in enumerate(far_blocks):
            stats_copy(layer, k, j, block, block).wait_recv()
            sums_copy(layer, k, j, block, block).wait_recv()
        rows = srecv[layer, k].reshape(S * STAT_ROWS, H)
        if S * STAT_ROWS < LANES:
            rows = jnp.concatenate([rows, jnp.zeros((LANES - S * STAT_ROWS, H), F32)], axis=0)
        stats = rows.T
        for h in range(heads):
            cols = slice(h * HD, (h + 1) * HD)
            tops = [stats[:, b * STAT_ROWS + 2 * h :][:, :1] for b in range(S)]
            highest = functools.reduce(jnp.maximum, tops)
            total = jnp.zeros((H, 1), F32)
            summed = jnp.zeros((H, HD), F32)
            for b in range(S):
                factor = jnp.exp(tops[b] - highest)
                total = total + factor * stats[:, b * STAT_ROWS + 2 * h + 1 :][:, :1]
                summed = summed + factor * orecv[layer, k, b, :, cols].astype(F32)
            att[k, :, cols] = (summed / total).astype(BF)
        rows = att[k]
        for ch in range(C):
            cols = slice(ch * DC, (ch + 1) * DC)
            pf[k, :, :, cols] = mm(rows, wo[layer, :, cols]).reshape(2, Rt, DC)
            p1s[layer, k, ch] = pf[k, other, :, cols].astype(BF)
            launch(pair_copy(layer, k, ch))

    def spread(layer, k):
        for ch in range(C):
            cols = slice(ch * DC, (ch + 1) * DC)
            pair_copy(layer, k, ch).wait_recv()
            chip_sum = pf[k, c, :, cols] + p1r[layer, k, ch].astype(F32)
            p2s[layer, k, ch] = chip_sum.astype(BF)
            for i in range(1, X):
                launch(chip_copy(layer, k, ch, x, chip_at(i)))
            residual[k, :, cols] = residual[k, :, cols] + chip_sum

    def settle(layer, k, gain):
        for ch in range(C):
            cols = slice(ch * DC, (ch + 1) * DC)
            for i in range(1, X):
                chip_copy(layer, k, ch, chip_at(i), chip_at(i)).wait_recv()
                residual[k, :, cols] = residual[k, :, cols] + p2r[
                    layer, k, ch, chip_at(i)
                ].astype(F32)
        share_rows(layer + 1, k, gain)

    def finish_read(layer, gain, follow):
        def close(k):
            with scope(f"settle{layer}{k}"):
                settle(layer, k, gain)
            with scope(f"follow{layer}{k}"):
                follow(k)

        for i, k in enumerate(order):
            with scope(f"combine{layer}{k}"):
                combine(layer, k)
            with scope(f"spread{layer}{k}"):
                spread(layer, k)
            if i:
                close(order[i - 1])
        close(order[-1])

    def turn_weight(src, dst):
        def one(j, carry):
            rows = pl.ds(pl.multiple_of(j * GROUP_ROWS, GROUP_ROWS), GROUP_ROWS)
            dst[rows] = src[:, rows].T
            return carry

        lax.fori_loop(0, D // GROUP_ROWS, one, 0)

    with scope("barrier"):
        pl.semaphore_wait(barrier, X + S - 1)
    load_t.wait()
    for i in range(1, X):
        launch(target_copy(x, chip_at(i)))
    for copy in load_kv[0]:
        copy.start()
    for copy in load_small:
        copy.wait()
    residual[x] = traw[x].astype(F32)
    share_rows(0, x, attend_gain[0:1])
    load_s.wait()
    with scope("norm_source"):
        for ch in range(NC):
            rows = sv[ch * RC : (ch + 1) * RC].astype(F32)
            xs[x, ch, c] = normed_rows(rows, source_gain[...]).astype(BF)
            for i in range(1, X):
                launch(source_copy(ch, x, chip_at(i)))
            launch(source_peer(ch, x, c))
    with scope("q0own"):
        load_q[0].wait()
        send_queries(0, x)
    for copy in load_kv[1]:
        copy.start()
    with scope("proj_chip0"):
        for ch in range(NC):
            source_peer(ch, x, other).wait_recv()
        for copy in load_kv[0]:
            copy.wait()
        project_chip(0, x)
    with scope("target_far"):
        for i in range(1, X):
            k = chip_at(i)
            target_copy(k, k).wait_recv()
            residual[k] = traw[k].astype(F32)
            share_rows(0, k, attend_gain[0:1])
    for copy in [load_q[1], *load_o]:
        copy.start()
    with scope("proj_chip1"):
        for copy in load_kv[1]:
            copy.wait()
        project_chip(1, x)
    with scope("q0far"):
        for i in range(1, X):
            send_queries(0, chip_at(i))
    for copy in [*load_late, *load_m]:
        copy.start()
    for ch in range(NC):
        with scope(f"forward{ch}"):
            for i in range(1, X):
                k = chip_at(i)
                source_copy(ch, k, k).wait_recv()
                launch(source_peer(ch, k, c))
        with scope(f"proj{ch}"):
            for i in range(1, X):
                source_peer(ch, chip_at(i), other).wait_recv()
                project_chunk(chip_at(i), ch)
    for k in order:
        with scope(f"attend0{k}"):
            attend(0, k)
    with scope("proj_rest"):
        for i in range(1, X):
            project_chip(1, chip_at(i))
    drain()
    for copy in [*load_o, load_q[1]]:
        copy.wait()
    finish_read(0, attend_gain[1:2], lambda k: send_queries(1, k))
    for copy in [*load_late, *load_m]:
        copy.wait()
    turns = [(wg, wgt), (wu, wut)]
    for i, k in enumerate(order):
        with scope(f"turn{i}"):
            for turn in turns[i * 2 // X : (i + 1) * 2 // X]:
                turn_weight(*turn)
        with scope(f"attend1{k}"):
            attend(1, k)
    pads = ((gpad, wgt), (upad, wut))

    def halo_out(number):
        return remote(
            hs.at[number],
            hr.at[number],
            h_send.at[number],
            h_recv.at[number],
            "sp",
            lax.rem(s + 1, S),
        )

    def lift(k):
        mixed = shared_rows(2, k)
        for number, (pad, weight) in enumerate(pads):
            lifted = mm(mixed, weight[...]).astype(BF).astype(F32)
            if k == X - 1:
                hs[number] = lifted[H - 8 :]

                @pl.when(s < S - 1)
                def _():
                    halo_out(number).start()

            pad[8 + k * H : 8 + (k + 1) * H] = lifted

    finish_read(1, mixer_gain[...], lift)

    def hidden_rows(start, stop):
        def convolved(pad, taps):
            return (
                taps[0:1] * pad[6 + start : 6 + stop]
                + taps[1:2] * pad[7 + start : 7 + stop]
                + taps[2:3] * pad[8 + start : 8 + stop]
            )

        gate = convolved(gpad, gate_taps)
        hid[start:stop] = (gate / (1.0 + jnp.exp(-gate)) * convolved(upad, up_taps)).astype(BF)

    with scope("hidden"):
        hidden_rows(16, T)

    @pl.when(s == 0)
    def _():
        for pad, _weight in pads:
            pad[:8] = jnp.zeros((8, F), F32)

    @pl.when(s > 0)
    def _():
        for number, (pad, _weight) in enumerate(pads):
            halo_out(number).wait_recv()
            pad[:8] = hr[number]

    @pl.when(s < S - 1)
    def _():
        for number in range(2):
            halo_out(number).wait_send()

    hidden_rows(0, 16)

    def down_pair(ch):
        return remote(d1s.at[ch], d1r.at[ch], d1_send.at[ch], d1_recv.at[ch], "tp", peer)

    def down_chip(ch, i, slot, where):
        return remote(
            d2s.at[ch, i],
            d2r.at[ch, slot],
            d2_send.at[ch, i],
            d2_recv.at[ch, slot],
            "tp",
            where * 2 + c,
        )

    with scope("down_mm"):
        rows = hid[...]
        for ch in range(C):
            cols = slice(ch * DC, (ch + 1) * DC)
            dpf[:, :, :, cols] = mm(rows, wd[:, cols]).reshape(X, 2, Rt, DC)
            d1s[ch] = dpf[:, other, :, cols].astype(BF)
            launch(down_pair(ch))
    with scope("down_pair"):
        for ch in range(C):
            cols = slice(ch * DC, (ch + 1) * DC)
            down_pair(ch).wait_recv()
            for i in range(1, X):
                k = chip_at(i)
                d2s[ch, i] = (dpf[k, c, :, cols] + d1r[ch, k].astype(F32)).astype(BF)
                launch(down_chip(ch, i, x, k))
            residual[x, :, cols] = (
                residual[x, :, cols] + dpf[x, c, :, cols] + d1r[ch, x].astype(F32)
            )
    with scope("drain"):
        last = [pending.pop() for _ in range(C * (X - 1))]
        drain()
    with scope("down_far"):
        for ch in range(C):
            cols = slice(ch * DC, (ch + 1) * DC)
            for i in range(1, X):
                k = chip_at(i)
                down_chip(ch, i, k, k).wait_recv()
                residual[x, :, cols] = residual[x, :, cols] + d2r[ch, k].astype(F32)
    result[...] = normed_rows(residual[x], final_gain[...]).astype(BF)
    for copy in last:
        copy.wait_send()


def body(n, S, *arrays):
    (
        source,
        target,
        source_gain,
        attend_gain,
        query_weight,
        key_weight,
        value_weight,
        out_weight,
        mixer_gain,
        gate_weight,
        up_weight,
        gate_taps,
        up_taps,
        down_weight,
        final_gain,
    ) = arrays
    Rs, D = source.shape
    Rt = target.shape[0]
    W = query_weight.shape[2]
    F = gate_weight.shape[1]
    T = n * Rt
    H = 2 * Rt
    X = n // 2
    NC = SOURCE_CHUNKS
    C = COLUMN_CHUNKS
    RC = Rs // NC
    DC = D // C
    hbm = pl.BlockSpec(memory_space=pl.ANY)
    dma = pltpu.SemaphoreType.DMA
    scratch = [
        pltpu.VMEM((1, D), F32),
        pltpu.VMEM((2, D), F32),
        pltpu.VMEM((1, D), F32),
        pltpu.VMEM((1, D), F32),
        pltpu.VMEM((3, F), F32),
        pltpu.VMEM((3, F), F32),
        pltpu.VMEM((Rs, D), BF),
        pltpu.VMEM((X, Rt, D), BF),
        pltpu.VMEM((2, D, W), BF),
        pltpu.VMEM((4, D, W), BF),
        pltpu.VMEM((2, W, D), BF),
        pltpu.VMEM((F, D), BF),
        pltpu.VMEM((F, D), BF),
        pltpu.VMEM((D, F), BF),
        pltpu.VMEM((D, F), BF),
        pltpu.VMEM((F, D), BF),
        pltpu.VMEM((X, NC, 2, RC, D), BF),
        pltpu.VMEM((3, X, 2, Rt, D), BF),
        pltpu.VMEM((4, X, NC, 2 * RC, W), BF),
        pltpu.VMEM((2, X, S, H, W), BF),
        pltpu.VMEM((2, X, S, H, W), BF),
        pltpu.VMEM((2, X, S, H, W), BF),
        pltpu.VMEM((2, X, S, STAT_ROWS, H), F32),
        pltpu.VMEM((2, X, S, STAT_ROWS, H), F32),
        pltpu.VMEM((X, 2, Rt, D), F32),
        pltpu.VMEM((X, H, W), BF),
        pltpu.VMEM((2, X, C, Rt, DC), BF),
        pltpu.VMEM((2, X, C, Rt, DC), BF),
        pltpu.VMEM((2, X, C, Rt, DC), BF),
        pltpu.VMEM((2, X, C, X, Rt, DC), BF),
        pltpu.VMEM((X, 2, Rt, D), F32),
        pltpu.VMEM((C, X, Rt, DC), BF),
        pltpu.VMEM((C, X, Rt, DC), BF),
        pltpu.VMEM((C, X, Rt, DC), BF),
        pltpu.VMEM((C, X, Rt, DC), BF),
        pltpu.VMEM((2, 8, F), F32),
        pltpu.VMEM((2, 8, F), F32),
        pltpu.VMEM((T + 8, F), F32),
        pltpu.VMEM((T + 8, F), F32),
        pltpu.VMEM((T, F), BF),
        pltpu.VMEM((X, Rt, D), F32),
        dma((22,)),
        dma((X,)),
        dma((X,)),
        dma((3, X)),
        dma((3, X)),
        dma((NC, X)),
        dma((NC, X)),
        dma((NC, X)),
        dma((NC, X)),
        dma((2, X, S)),
        dma((2, X, S)),
        dma((2, X, S)),
        dma((2, X, S)),
        dma((2, X, S)),
        dma((2, X, S)),
        dma((2, X, C)),
        dma((2, X, C)),
        dma((2, X, C, X)),
        dma((2, X, C, X)),
        dma((C,)),
        dma((C,)),
        dma((C, X)),
        dma((C, X)),
        dma((2,)),
        dma((2,)),
    ]
    return pl.pallas_call(
        functools.partial(kernel, n, S),
        out_shape=pltpu.VMEM((Rt, D), BF),
        in_specs=[hbm] * 15,
        out_specs=pl.BlockSpec(memory_space=pltpu.VMEM),
        scratch_shapes=scratch,
        compiler_params=pltpu.CompilerParams(
            collective_id=0, has_side_effects=True, vmem_limit_bytes=66000000
        ),
    )(
        source,
        target,
        source_gain.reshape(1, D),
        attend_gain,
        query_weight,
        key_weight,
        value_weight,
        out_weight,
        mixer_gain.reshape(1, D),
        gate_weight.T,
        up_weight.T,
        gate_taps,
        up_taps,
        down_weight,
        final_gain.reshape(1, D),
    )


def solution(mesh):
    placed = (
        P(("grp", "sp", "tp"), None),
        P(("grp", "sp", "tp"), None),
        P(),
        P(),
        P(None, None, "tp"),
        P(None, None, "tp"),
        P(None, None, "tp"),
        P(None, "tp", None),
        P(),
        P(None, "tp"),
        P(None, "tp"),
        P(None, "tp"),
        P(None, "tp"),
        P("tp", None),
        P(),
    )
    return jax.shard_map(
        functools.partial(body, mesh.shape["tp"], mesh.shape["sp"]),
        mesh=mesh,
        in_specs=placed,
        out_specs=P(("grp", "sp", "tp"), None),
        check_vma=False,
    )
```

```python
import functools

import jax
import jax.numpy as jnp
from jax import lax
from jax.experimental import pallas as pl
from jax.experimental.pallas import tpu as pltpu
from jax.sharding import PartitionSpec as P

HD = 256
EPS = 1e-06
STAT_ROWS = 8
LANES = 128
SOURCE_CHUNKS = 4
STREAMS_PER_CHIP = 2
OUT_CHUNKS = 2
DOWN_CHUNKS = 4
GROUP_ROWS = 256
MESH = pl.DeviceIdType.MESH
BF = jnp.bfloat16
F32 = jnp.float32


def normed_rows(wide, gain):
    return wide * lax.rsqrt(jnp.mean(wide * wide, axis=-1, keepdims=True) + EPS) * gain


def mm(a, b):
    return jnp.dot(a, b, preferred_element_type=F32)


def scope(name):
    return jax.named_scope(name)


def kernel(
    n,
    S,
    source,
    target,
    source_gain_in,
    attend_gain_in,
    query_weight,
    key_weight,
    value_weight,
    out_weight,
    mixer_gain_in,
    gate_weight,
    up_weight,
    gate_taps_in,
    up_taps_in,
    down_weight,
    final_gain_in,
    result,
    source_gain,
    attend_gain,
    mixer_gain,
    final_gain,
    gate_taps,
    up_taps,
    sv,
    traw,
    wq,
    wkv,
    wo,
    wg,
    wu,
    wgt,
    wut,
    wd,
    xs,
    xt,
    kv,
    qall,
    osend,
    orecv,
    ssend,
    srecv,
    pf,
    att,
    p1s,
    p1r,
    p2s,
    p2r,
    dpf,
    d1s,
    d1r,
    d2s,
    d2r,
    hs,
    hr,
    gpad,
    upad,
    hid,
    residual,
    load_sem,
    sent,
    tr_recv,
    n_recv,
    sx_recv,
    sd_recv,
    own_recv,
    q_recv,
    cross_recv,
    r_recv,
    s_recv,
    p1_recv,
    p2_recv,
    d1_recv,
    d2_recv,
    h_recv,
):
    X = n // 2
    Rs, D = source.shape
    Rt = target.shape[0]
    W = wq.shape[2]
    T = n * Rt
    NS, Rh = residual.shape[:2]
    SUB = NS // X
    H = 2 * Rh
    heads = W // HD
    F = wg.shape[0]
    NC = xs.shape[1]
    RC = Rs // NC
    C = p1s.shape[2]
    C2 = d1s.shape[0]
    scale = HD ** (-0.5)
    t = lax.axis_index("tp")
    s = lax.axis_index("sp")
    x = lax.div(t, 2)
    c = lax.rem(t, 2)
    other = 1 - c
    peer = x * 2 + other
    offsets = range(1, X)
    order = [k * SUB + h for k in reversed(range(X)) for h in range(SUB)]

    def to_chip(i):
        return lax.rem(x + i, X)

    def from_chip(i):
        return lax.rem(x + X - i, X)

    def streams(k):
        return pl.ds(k * SUB, SUB)

    def remote(src, dst, ss, rs, axis, where):
        return pltpu.make_async_remote_copy(
            src_ref=src,
            dst_ref=dst,
            send_sem=ss,
            recv_sem=rs,
            device_id={axis: where},
            device_id_type=MESH,
        )

    def wait_for(sem, ref):
        remote(ref, ref, sent.at[0], sem, "tp", peer).wait_recv()

    def wait_sent(number, ref):
        remote(ref, ref, sent.at[number], own_recv.at[0], "tp", peer).wait_send()

    far_blocks = []
    low = s * 0
    high = low + (S - 1)
    for _ in range(S - 1):
        left = lax.div(2 * s - low - high + S, S)
        far_blocks.append(left * low + (1 - left) * high)
        low = low + left
        high = high - (1 - left)
    most = pl.ds(0, S - 1)
    half = S // 2
    RELAY = S % 2 == 0 and S > 2

    barrier = pltpu.get_barrier_semaphore()
    pl.semaphore_signal(barrier, inc=1, device_id={"tp": peer}, device_id_type=MESH)
    for i in offsets:
        pl.semaphore_signal(
            barrier, inc=1, device_id={"tp": to_chip(i) * 2 + c}, device_id_type=MESH
        )
    for block in far_blocks:
        pl.semaphore_signal(barrier, inc=1, device_id={"sp": block}, device_id_type=MESH)

    def load(number, src, dst):
        return pltpu.make_async_copy(src, dst, load_sem.at[number])

    load_t = load(0, target, traw.at[x])
    load_s = load(1, source, sv)
    load_small = [load(2, attend_gain_in, attend_gain), load(3, source_gain_in, source_gain)]
    load_late = [
        load(0, mixer_gain_in, mixer_gain),
        load(1, final_gain_in, final_gain),
        load(2, gate_taps_in, gate_taps),
        load(3, up_taps_in, up_taps),
    ]
    load_q = [load(4, query_weight.at[l], wq.at[l]) for l in range(2)]
    load_kv = [
        [
            load(5 + 2 * l, key_weight.at[l], wkv.at[2 * l]),
            load(6 + 2 * l, value_weight.at[l], wkv.at[2 * l + 1]),
        ]
        for l in range(2)
    ]
    load_o = [load(5 + l, out_weight.at[l], wo.at[l]) for l in range(2)]
    load_m = [load(9, gate_weight, wg), load(10, up_weight, wu), load(11, down_weight, wd)]
    for copy in [load_t, *load_small, load_s, load_q[0]]:
        copy.start()

    def share_rows(a, rows, number):
        remote(
            xt.at[a, rows, c], xt.at[a, rows, c], sent.at[1], n_recv.at[a, number], "tp", peer
        ).start()

    def await_rows(a, rows, number):
        wait_for(n_recv.at[a, number], xt.at[a, rows, other])

    def first_rows(k):
        rows = traw[k].astype(F32)
        residual[streams(k)] = rows.reshape(SUB, Rh, D)
        xt[0, streams(k), c] = normed_rows(rows, attend_gain[0:1]).astype(BF).reshape(SUB, Rh, D)
        share_rows(0, streams(k), k)

    def first_queries(k):
        await_rows(0, streams(k), k)
        rows = xt[0, streams(k)].reshape(SUB * H, D)
        qall[0, streams(k), s] = mm(rows, wq[0]).astype(BF).reshape(SUB, H, W)
        for block in far_blocks:
            mine = qall.at[0, streams(k), s]
            remote(mine, mine, sent.at[4], q_recv.at[0, k], "sp", block).start()

    def next_queries(j):
        await_rows(1, j, j)
        qall[1, j, s] = mm(xt[1, j].reshape(H, D), wq[1]).astype(BF)
        if RELAY:
            mine = qall.at[1, j, s]
            remote(mine, mine, sent.at[4], cross_recv.at[j], "sp", lax.rem(s + half, S)).start()
            to_mates(j, s)
        else:
            for block in far_blocks:
                mine = qall.at[1, j, s]
                remote(mine, mine, sent.at[4], q_recv.at[1, j], "sp", block).start()

    def to_mates(j, block):
        for m in range(1, half):
            mate = lax.div(s, half) * half + lax.rem(s + m, half)
            rows = qall.at[1, j, block]
            remote(rows, rows, sent.at[4], q_recv.at[1, j], "sp", mate).start()

    def relay(j):
        if RELAY:
            block = lax.rem(s + half, S)
            wait_for(cross_recv.at[j], qall.at[1, j, block])
            to_mates(j, block)

    def await_queries(j):
        count = 2 * (half - 1) if RELAY else S - 1
        wait_for(q_recv.at[1, j], qall.at[1, j, pl.ds(0, count)])

    def project_chip(layer, k):
        rows = xs[k].reshape(2 * Rs, D)

        def one(j, carry):
            kv[j, k] = mm(rows, wkv[j]).astype(BF).reshape(NC, 2 * RC, W)
            return carry

        lax.fori_loop(2 * layer, 2 * layer + 2, one, 0)

    def project_chunk(k, ch):
        rows = xs[k, ch].reshape(2 * RC, D)

        def one(j, carry):
            kv[j, k, ch] = mm(rows, wkv[j]).astype(BF)
            return carry

        lax.fori_loop(0, 2, one, 0)

    G = max(1, min(S, GROUP_ROWS // H))
    while S % G:
        G -= 1

    def attend(layer, j):
        def group(base):
            blocks = pl.ds(base, G)
            lanes = lax.broadcasted_iota(jnp.int32, (G * H, LANES), 1)
            packed = jnp.zeros((G * H, LANES), F32)
            for h in range(heads):
                cols = slice(h * HD, (h + 1) * HD)
                query = qall[layer, j, blocks, :, cols].reshape(G * H, HD)
                keys = kv[2 * layer, :, :, :, cols].reshape(n * Rs, HD)
                values = kv[2 * layer + 1, :, :, :, cols].reshape(n * Rs, HD)
                scores = (
                    lax.dot_general(
                        query, keys, (((1,), (1,)), ((), ())), preferred_element_type=F32
                    )
                    * scale
                )
                top = jnp.max(scores, axis=-1, keepdims=True)
                raised = jnp.exp(scores - top)
                total = jnp.sum(raised, axis=-1, keepdims=True)
                osend[layer, j, blocks, :, cols] = (
                    mm(raised.astype(BF), values).astype(BF).reshape(G, H, HD)
                )
                packed = jnp.where(lanes == 2 * h, top, packed)
                packed = jnp.where(lanes == 2 * h + 1, total, packed)
            stats = packed.T[:STAT_ROWS]
            for b in range(G):
                ssend[layer, j, base + b] = stats[:, b * H : (b + 1) * H]

        if G == S:
            group(0)
        else:

            def one(g, carry):
                group(g * G)
                return carry

            lax.fori_loop(0, S // G, one, 0)
        for block in far_blocks:
            for src, dst, number, sem in (
                (ssend, srecv, 6, s_recv),
                (osend, orecv, 5, r_recv),
            ):
                remote(
                    src.at[layer, j, block],
                    dst.at[layer, j, s],
                    sent.at[number],
                    sem.at[layer, j],
                    "sp",
                    block,
                ).start()
        orecv[layer, j, s] = osend[layer, j, s]
        srecv[layer, j, s] = ssend[layer, j, s]

    def combine(layer, j):
        wait_for(s_recv.at[layer, j], srecv.at[layer, j, most])
        wait_for(r_recv.at[layer, j], orecv.at[layer, j, most])
        rows = srecv[layer, j].reshape(S * STAT_ROWS, H)
        if S * STAT_ROWS < LANES:
            rows = jnp.concatenate([rows, jnp.zeros((LANES - S * STAT_ROWS, H), F32)], axis=0)
        stats = rows.T
        for h in range(heads):
            cols = slice(h * HD, (h + 1) * HD)
            tops = [stats[:, b * STAT_ROWS + 2 * h :][:, :1] for b in range(S)]
            highest = functools.reduce(jnp.maximum, tops)
            total = jnp.zeros((H, 1), F32)
            summed = jnp.zeros((H, HD), F32)
            for b in range(S):
                factor = jnp.exp(tops[b] - highest)
                total = total + factor * stats[:, b * STAT_ROWS + 2 * h + 1 :][:, :1]
                summed = summed + factor * orecv[layer, j, b, :, cols].astype(F32)
            att[j, :, cols] = (summed / total).astype(BF)
        rows = att[j]
        for ch in range(C):
            cols = slice(ch * (D // C), (ch + 1) * (D // C))
            pf[j, :, :, cols] = mm(rows, wo[layer, :, cols]).reshape(2, Rh, D // C)
            p1s[layer, j, ch] = pf[j, other, :, cols].astype(BF)
            remote(
                p1s.at[layer, j, ch],
                p1r.at[layer, j, ch],
                sent.at[7],
                p1_recv.at[layer, j, ch],
                "tp",
                peer,
            ).start()

    def spread(layer, j):
        for ch in range(C):
            cols = slice(ch * (D // C), (ch + 1) * (D // C))
            wait_for(p1_recv.at[layer, j, ch], p1r.at[layer, j, ch])
            chip_sum = pf[j, c, :, cols] + p1r[layer, j, ch].astype(F32)
            p2s[layer, j, ch] = chip_sum.astype(BF)
            for i in offsets:
                remote(
                    p2s.at[layer, j, ch],
                    p2r.at[layer, j, ch, i - 1],
                    sent.at[8],
                    p2_recv.at[layer, j, ch, i - 1],
                    "tp",
                    to_chip(i) * 2 + c,
                ).start()
            residual[j, :, cols] = residual[j, :, cols] + chip_sum

    def settle(layer, j, gain):
        for ch in range(C):
            cols = slice(ch * (D // C), (ch + 1) * (D // C))
            for i in offsets:
                wait_for(p2_recv.at[layer, j, ch, i - 1], p2r.at[layer, j, ch, i - 1])
                residual[j, :, cols] = residual[j, :, cols] + p2r[layer, j, ch, i - 1].astype(F32)
        xt[layer + 1, j, c] = normed_rows(residual[j], gain).astype(BF)
        share_rows(layer + 1, j, j)

    def turn_weight(src, dst):
        def one(j, carry):
            rows = pl.ds(pl.multiple_of(j * GROUP_ROWS, GROUP_ROWS), GROUP_ROWS)
            dst[rows] = src[:, rows].T
            return carry

        lax.fori_loop(0, D // GROUP_ROWS, one, 0)

    with scope("barrier"):
        pl.semaphore_wait(barrier, X + S - 1)
    load_t.wait()
    for i in offsets:
        remote(
            traw.at[x], traw.at[x], sent.at[0], tr_recv.at[i - 1], "tp", to_chip(i) * 2 + c
        ).start()
    for copy in load_kv[0]:
        copy.start()
    for copy in load_small:
        copy.wait()
    first_rows(x)
    load_s.wait()
    with scope("norm_source"):
        for ch in range(NC):
            rows = sv[ch * RC : (ch + 1) * RC].astype(F32)
            xs[x, ch, c] = normed_rows(rows, source_gain[...]).astype(BF)
            mine = xs.at[x, ch, c]
            for i in offsets:
                remote(
                    mine, mine, sent.at[2], sx_recv.at[ch, i - 1], "tp", to_chip(i) * 2 + c
                ).start()
            remote(mine, mine, sent.at[3], own_recv.at[0], "tp", peer).start()
    with scope("q0own"):
        load_q[0].wait()
        first_queries(x)
    for copy in [*load_kv[1], *load_m, *load_late]:
        copy.start()
    with scope("proj_chip0"):
        wait_for(own_recv.at[0], xs.at[x, :, other])
        for copy in load_kv[0]:
            copy.wait()
        project_chip(0, x)
    with scope("target_far"):
        for i in offsets:
            k = from_chip(i)
            wait_for(tr_recv.at[i - 1], traw.at[k])
            first_rows(k)
    for copy in [load_q[1], *load_o]:
        copy.start()
    with scope("proj_chip1"):
        for copy in load_kv[1]:
            copy.wait()
        project_chip(1, x)
    with scope("q0far"):
        for i in offsets:
            first_queries(from_chip(i))
    turns = [(load_m[0], wg, wgt), (load_m[1], wu, wut)]
    for ch in range(NC):
        if ch and turns:
            with scope("turn"):
                copy, src, dst = turns.pop(0)
                copy.wait()
                turn_weight(src, dst)
        with scope(f"forward{ch}"):
            for i in offsets:
                landed = xs.at[from_chip(i), ch, c]
                wait_for(sx_recv.at[ch, i - 1], landed)
                remote(landed, landed, sent.at[3], sd_recv.at[ch, i - 1], "tp", peer).start()
        with scope(f"proj{ch}"):
            for i in offsets:
                wait_for(sd_recv.at[ch, i - 1], xs.at[from_chip(i), ch, other])
                project_chunk(from_chip(i), ch)
    for k in range(X):
        wait_for(q_recv.at[0, k], qall.at[0, streams(k), most])
    for j in order:
        with scope(f"attend0{j}"):
            attend(0, j)
    with scope("proj_rest"):
        for i in offsets:
            project_chip(1, from_chip(i))
    for copy in [*load_o, load_q[1], *load_late, load_m[2]]:
        copy.wait()
    for i in range(NS + 2):
        if i < NS:
            with scope(f"combine0{i}"):
                combine(0, order[i])
        if i >= 2:
            with scope(f"query{i - 2}"):
                next_queries(order[i - 2])
        if i >= 4:
            with scope(f"relay{i - 4}"):
                relay(order[i - 4])
        if i < NS:
            with scope(f"spread0{i}"):
                spread(0, order[i])
        if 1 <= i <= NS:
            with scope(f"settle0{i - 1}"):
                settle(0, order[i - 1], attend_gain[1:2])
    for a in range(NS):
        for i in range(NS - 2 + a, min(NS, NS - 1 + a)):
            with scope(f"relay{i}"):
                relay(order[i])
        with scope(f"attend1{a}"):
            await_queries(order[a])
            attend(1, order[a])
    pads = ((gpad, wgt), (upad, wut))

    def halo_out(number):
        return remote(
            hs.at[number],
            hr.at[number],
            sent.at[11 + number],
            h_recv.at[number],
            "sp",
            lax.rem(s + 1, S),
        )

    def lift(k):
        for h in range(SUB):
            await_rows(2, k * SUB + h, k * SUB + h)
        mixed = xt[2, streams(k)].reshape(SUB * H, D)
        for number, (pad, weight) in enumerate(pads):
            lifted = mm(mixed, weight[...]).astype(BF).astype(F32)
            if k == X - 1:
                hs[number] = lifted[SUB * H - 8 :]

                @pl.when(s < S - 1)
                def _():
                    halo_out(number).start()

            for piece in range(2 * SUB):
                part, core = divmod(piece, 2)
                start = 8 + (2 * k + core) * Rt + part * Rh
                pad[start : start + Rh] = lifted[piece * Rh : (piece + 1) * Rh]

    lifts = [*reversed(range(X))]
    for i in range(NS + 1):
        if i < NS:
            with scope(f"combine1{i}"):
                combine(1, order[i])
            with scope(f"spread1{i}"):
                spread(1, order[i])
            if i > SUB and (i - 1) % SUB == 0:
                with scope(f"lift{i}"):
                    lift(lifts.pop(0))
        if i >= 1:
            with scope(f"settle1{i - 1}"):
                settle(1, order[i - 1], mixer_gain[...])
    with scope("lift"):
        for k in lifts:
            lift(k)

    def hidden_rows(start, stop):
        def convolved(pad, taps):
            return (
                taps[0:1] * pad[6 + start : 6 + stop]
                + taps[1:2] * pad[7 + start : 7 + stop]
                + taps[2:3] * pad[8 + start : 8 + stop]
            )

        gate = convolved(gpad, gate_taps)
        hid[start:stop] = (gate / (1.0 + jnp.exp(-gate)) * convolved(upad, up_taps)).astype(BF)

    with scope("hidden"):
        hidden_rows(16, T)

    @pl.when(s == 0)
    def _():
        for pad, _weight in pads:
            pad[:8] = jnp.zeros((8, F), F32)

    @pl.when(s > 0)
    def _():
        for number, (pad, _weight) in enumerate(pads):
            halo_out(number).wait_recv()
            pad[:8] = hr[number]

    @pl.when(s < S - 1)
    def _():
        for number in range(2):
            halo_out(number).wait_send()

    hidden_rows(0, 16)

    def down_cols(ch):
        return slice(ch * (D // C2), (ch + 1) * (D // C2))

    with scope("down_mm"):
        rows = hid[...]
        for ch in range(C2):
            dpf[:, :, :, down_cols(ch)] = mm(rows, wd[:, down_cols(ch)]).reshape(
                X, 2, Rt, D // C2
            )
            d1s[ch] = dpf[:, other, :, down_cols(ch)].astype(BF)
            remote(d1s.at[ch], d1r.at[ch], sent.at[9], d1_recv.at[ch], "tp", peer).start()
    own = streams(x)
    with scope("down_pair"):
        for ch in range(C2):
            cols = down_cols(ch)
            wait_for(d1_recv.at[ch], d1r.at[ch])
            for i in offsets:
                k = to_chip(i)
                d2s[ch, i - 1] = (dpf[k, c, :, cols] + d1r[ch, k].astype(F32)).astype(BF)
                remote(
                    d2s.at[ch, i - 1],
                    d2r.at[ch, i - 1],
                    sent.at[10],
                    d2_recv.at[ch, i - 1],
                    "tp",
                    k * 2 + c,
                ).start()
            added = dpf[x, c, :, cols] + d1r[ch, x].astype(F32)
            residual[own, :, cols] = residual[own, :, cols] + added.reshape(SUB, Rh, D // C2)
    with scope("drain"):
        first = pl.ds(0, X - 1)
        wait_sent(0, traw.at[first])
        wait_sent(1, xt.at[:, :, 0])
        wait_sent(2, xs.at[first, :, 0])
        wait_sent(3, xs.at[:, :, 0])
        wait_sent(4, qall.at[:, :, most])
        wait_sent(5, osend.at[:, :, most])
        wait_sent(6, ssend.at[:, :, most])
        wait_sent(7, p1s)
        wait_sent(8, p2r)
        wait_sent(9, d1s)
    with scope("down_far"):
        for ch in range(C2):
            cols = down_cols(ch)
            for i in offsets:
                wait_for(d2_recv.at[ch, i - 1], d2r.at[ch, i - 1])
                added = d2r[ch, i - 1].astype(F32)
                residual[own, :, cols] = residual[own, :, cols] + added.reshape(SUB, Rh, D // C2)
    result[...] = normed_rows(residual[own].reshape(Rt, D), final_gain[...]).astype(BF)
    wait_sent(10, d2s)


def body(n, S, *arrays):
    (
        source,
        target,
        source_gain,
        attend_gain,
        query_weight,
        key_weight,
        value_weight,
        out_weight,
        mixer_gain,
        gate_weight,
        up_weight,
        gate_taps,
        up_taps,
        down_weight,
        final_gain,
    ) = arrays
    Rs, D = source.shape
    Rt = target.shape[0]
    W = query_weight.shape[2]
    F = gate_weight.shape[1]
    T = n * Rt
    X = n // 2
    SUB = STREAMS_PER_CHIP
    NS = SUB * X
    Rh = Rt // SUB
    H = 2 * Rh
    NC = SOURCE_CHUNKS
    C = OUT_CHUNKS
    C2 = DOWN_CHUNKS
    RC = Rs // NC
    hbm = pl.BlockSpec(memory_space=pl.ANY)
    dma = pltpu.SemaphoreType.DMA
    scratch = [
        pltpu.VMEM((1, D), F32),
        pltpu.VMEM((2, D), F32),
        pltpu.VMEM((1, D), F32),
        pltpu.VMEM((1, D), F32),
        pltpu.VMEM((3, F), F32),
        pltpu.VMEM((3, F), F32),
        pltpu.VMEM((Rs, D), BF),
        pltpu.VMEM((X, Rt, D), BF),
        pltpu.VMEM((2, D, W), BF),
        pltpu.VMEM((4, D, W), BF),
        pltpu.VMEM((2, W, D), BF),
        pltpu.VMEM((F, D), BF),
        pltpu.VMEM((F, D), BF),
        pltpu.VMEM((D, F), BF),
        pltpu.VMEM((D, F), BF),
        pltpu.VMEM((F, D), BF),
        pltpu.VMEM((X, NC, 2, RC, D), BF),
        pltpu.VMEM((3, NS, 2, Rh, D), BF),
        pltpu.VMEM((4, X, NC, 2 * RC, W), BF),
        pltpu.VMEM((2, NS, S, H, W), BF),
        pltpu.VMEM((2, NS, S, H, W), BF),
        pltpu.VMEM((2, NS, S, H, W), BF),
        pltpu.VMEM((2, NS, S, STAT_ROWS, H), F32),
        pltpu.VMEM((2, NS, S, STAT_ROWS, H), F32),
        pltpu.VMEM((NS, 2, Rh, D), F32),
        pltpu.VMEM((NS, H, W), BF),
        pltpu.VMEM((2, NS, C, Rh, D // C), BF),
        pltpu.VMEM((2, NS, C, Rh, D // C), BF),
        pltpu.VMEM((2, NS, C, Rh, D // C), BF),
        pltpu.VMEM((2, NS, C, X - 1, Rh, D // C), BF),
        pltpu.VMEM((X, 2, Rt, D), F32),
        pltpu.VMEM((C2, X, Rt, D // C2), BF),
        pltpu.VMEM((C2, X, Rt, D // C2), BF),
        pltpu.VMEM((C2, X - 1, Rt, D // C2), BF),
        pltpu.VMEM((C2, X - 1, Rt, D // C2), BF),
        pltpu.VMEM((2, 8, F), F32),
        pltpu.VMEM((2, 8, F), F32),
        pltpu.VMEM((T + 8, F), F32),
        pltpu.VMEM((T + 8, F), F32),
        pltpu.VMEM((T, F), BF),
        pltpu.VMEM((NS, Rh, D), F32),
        dma((12,)),
        dma((13,)),
        dma((X - 1,)),
        dma((3, NS)),
        dma((NC, X - 1)),
        dma((NC, X - 1)),
        dma((1,)),
        dma((2, NS)),
        dma((NS,)),
        dma((2, NS)),
        dma((2, NS)),
        dma((2, NS, C)),
        dma((2, NS, C, X - 1)),
        dma((C2,)),
        dma((C2, X - 1)),
        dma((2,)),
    ]
    return pl.pallas_call(
        functools.partial(kernel, n, S),
        out_shape=pltpu.VMEM((Rt, D), BF),
        in_specs=[hbm] * 15,
        out_specs=pl.BlockSpec(memory_space=pltpu.VMEM),
        scratch_shapes=scratch,
        compiler_params=pltpu.CompilerParams(
            collective_id=0, has_side_effects=True, vmem_limit_bytes=66000000
        ),
    )(
        source,
        target,
        source_gain.reshape(1, D),
        attend_gain,
        query_weight,
        key_weight,
        value_weight,
        out_weight,
        mixer_gain.reshape(1, D),
        gate_weight.T,
        up_weight.T,
        gate_taps,
        up_taps,
        down_weight,
        final_gain.reshape(1, D),
    )


def solution(mesh):
    placed = (
        P(("grp", "sp", "tp"), None),
        P(("grp", "sp", "tp"), None),
        P(),
        P(),
        P(None, None, "tp"),
        P(None, None, "tp"),
        P(None, None, "tp"),
        P(None, "tp", None),
        P(),
        P(None, "tp"),
        P(None, "tp"),
        P(None, "tp"),
        P(None, "tp"),
        P("tp", None),
        P(),
    )
    return jax.shard_map(
        functools.partial(body, mesh.shape["tp"], mesh.shape["sp"]),
        mesh=mesh,
        in_specs=placed,
        out_specs=P(("grp", "sp", "tp"), None),
        check_vma=False,
    )
```

```python
import functools

import jax
import jax.numpy as jnp
from jax import lax
from jax.experimental import pallas as pl
from jax.experimental.pallas import tpu as pltpu
from jax.sharding import PartitionSpec as P

HD = 256
EPS = 1e-06
LANES = 128
SOURCE_CHUNKS = 4
STREAMS_PER_CHIP = 2
RELAYED = (2,)
EARLY = 1
STEPS = (
    "a1",
    "r2",
    "c0",
    "a2",
    "s0",
    "a3",
    "c1",
    "s1",
    "e0",
    "c2",
    "s2",
    "e1",
    "c3",
    "s3",
    "l0",
    "e2",
    "e3",
    "l1",
)
OUT_CHUNKS = 2
DOWN_CHUNKS = 4
GROUP_ROWS = 256
MESH = pl.DeviceIdType.MESH
BF = jnp.bfloat16
F32 = jnp.float32


def normed_rows(wide, gain):
    return wide * lax.rsqrt(jnp.mean(wide * wide, axis=-1, keepdims=True) + EPS) * gain


def mm(a, b):
    return jnp.dot(a, b, preferred_element_type=F32)


def scope(name):
    return jax.named_scope(name)


def kernel(
    n,
    S,
    source,
    target,
    source_gain_in,
    attend_gain_in,
    query_weight,
    key_weight,
    value_weight,
    out_weight,
    mixer_gain_in,
    gate_weight,
    up_weight,
    gate_taps_in,
    up_taps_in,
    down_weight,
    final_gain_in,
    result,
    source_gain,
    attend_gain,
    mixer_gain,
    final_gain,
    gate_taps,
    up_taps,
    sv,
    traw,
    wq,
    wkv,
    wo,
    wg,
    wu,
    wgt,
    wut,
    wd,
    xs,
    xt,
    kv,
    qall,
    osend,
    orecv,
    ssend,
    srecv,
    pf,
    att,
    p1s,
    p1r,
    p2s,
    p2r,
    dpf,
    d1s,
    d1r,
    d2s,
    d2r,
    hs,
    hr,
    gpad,
    upad,
    hid,
    residual,
    load_sem,
    sent,
    tr_recv,
    n_recv,
    sx_recv,
    sd_recv,
    own_recv,
    q_recv,
    cross_recv,
    r_recv,
    s_recv,
    p1_recv,
    p2_recv,
    d1_recv,
    d2_recv,
    h_recv,
):
    X = n // 2
    Rs, D = source.shape
    Rt = target.shape[0]
    W = wq.shape[2]
    T = n * Rt
    NS, Rh = residual.shape[:2]
    SUB = NS // X
    H = 2 * Rh
    heads = W // HD
    F = wg.shape[0]
    NC = xs.shape[1]
    RC = Rs // NC
    C = p1s.shape[2]
    C2 = d1s.shape[0]
    scale = HD ** (-0.5)
    t = lax.axis_index("tp")
    s = lax.axis_index("sp")
    x = lax.div(t, 2)
    c = lax.rem(t, 2)
    other = 1 - c
    peer = x * 2 + other
    offsets = range(1, X)
    order = [k * SUB + h for k in reversed(range(X)) for h in range(SUB)]

    def to_chip(i):
        return lax.rem(x + i, X)

    def from_chip(i):
        return lax.rem(x + X - i, X)

    def streams(k):
        return pl.ds(k * SUB, SUB)

    def remote(src, dst, ss, rs, axis, where):
        return pltpu.make_async_remote_copy(
            src_ref=src,
            dst_ref=dst,
            send_sem=ss,
            recv_sem=rs,
            device_id={axis: where},
            device_id_type=MESH,
        )

    def wait_for(sem, ref):
        remote(ref, ref, sent.at[0], sem, "tp", peer).wait_recv()

    def wait_sent(number, ref):
        remote(ref, ref, sent.at[number], own_recv.at[0], "tp", peer).wait_send()

    far_blocks = []
    low = s * 0
    high = low + (S - 1)
    for _ in range(S - 1):
        left = lax.div(2 * s - low - high + S, S)
        far_blocks.append(left * low + (1 - left) * high)
        low = low + left
        high = high - (1 - left)
    most = pl.ds(0, S - 1)
    half = S // 2
    RELAY = S % 2 == 0 and S > 2

    barrier = pltpu.get_barrier_semaphore()
    pl.semaphore_signal(barrier, inc=1, device_id={"tp": peer}, device_id_type=MESH)
    for i in offsets:
        pl.semaphore_signal(
            barrier, inc=1, device_id={"tp": to_chip(i) * 2 + c}, device_id_type=MESH
        )
    for block in far_blocks:
        pl.semaphore_signal(barrier, inc=1, device_id={"sp": block}, device_id_type=MESH)

    def load(number, src, dst):
        return pltpu.make_async_copy(src, dst, load_sem.at[number])

    load_t = load(0, target, traw.at[x])
    load_s = load(1, source, sv)
    load_small = [load(2, attend_gain_in, attend_gain), load(3, source_gain_in, source_gain)]
    load_late = [
        load(0, mixer_gain_in, mixer_gain),
        load(1, final_gain_in, final_gain),
        load(2, gate_taps_in, gate_taps),
        load(3, up_taps_in, up_taps),
    ]
    load_q = [load(4, query_weight.at[l], wq.at[l]) for l in range(2)]
    load_kv = [
        [
            load(5 + 2 * l, key_weight.at[l], wkv.at[2 * l]),
            load(6 + 2 * l, value_weight.at[l], wkv.at[2 * l + 1]),
        ]
        for l in range(2)
    ]
    load_o = [load(5 + l, out_weight.at[l], wo.at[l]) for l in range(2)]
    load_m = [load(9, gate_weight, wg), load(10, up_weight, wu), load(11, down_weight, wd)]
    for copy in [load_t, *load_small, load_s, load_q[0]]:
        copy.start()

    def share_rows(a, rows, number):
        remote(
            xt.at[a, rows, c], xt.at[a, rows, c], sent.at[1], n_recv.at[number], "tp", peer
        ).start()

    def await_rows(a, rows, number):
        wait_for(n_recv.at[number], xt.at[a, rows, other])

    def first_rows(k):
        rows = traw[k].astype(F32)
        residual[streams(k)] = rows.reshape(SUB, Rh, D)
        xt[0, streams(k), c] = normed_rows(rows, attend_gain[0:1]).astype(BF).reshape(SUB, Rh, D)
        share_rows(0, streams(k), k)

    def first_queries(k):
        await_rows(0, streams(k), k)
        rows = xt[0, streams(k)].reshape(SUB * H, D)
        qall[0, streams(k), s] = mm(rows, wq[0]).astype(BF).reshape(SUB, H, W)
        for block in far_blocks:
            mine = qall.at[0, streams(k), s]
            remote(mine, mine, sent.at[4], q_recv.at[k], "sp", block).start()

    def next_queries(j):
        await_rows(1, j, j)
        qall[1, j, s] = mm(xt[1, j].reshape(H, D), wq[1]).astype(BF)
        if relayed(j):
            mine = qall.at[1, j, s]
            remote(mine, mine, sent.at[4], cross_recv.at[j], "sp", lax.rem(s + half, S)).start()
            to_mates(j, s)
        else:
            for block in far_blocks:
                mine = qall.at[1, j, s]
                remote(mine, mine, sent.at[4], q_recv.at[j], "sp", block).start()

    def to_mates(j, block):
        for m in range(1, half):
            mate = lax.div(s, half) * half + lax.rem(s + m, half)
            rows = qall.at[1, j, block]
            remote(rows, rows, sent.at[4], q_recv.at[j], "sp", mate).start()

    def relayed(j):
        return RELAY and order.index(j) in RELAYED

    def relay(j):
        if relayed(j):
            block = lax.rem(s + half, S)
            wait_for(cross_recv.at[j], qall.at[1, j, block])
            to_mates(j, block)

    def await_queries(j):
        count = 2 * (half - 1) if relayed(j) else S - 1
        wait_for(q_recv.at[j], qall.at[1, j, pl.ds(0, count)])

    def project_chip(layer, k):
        rows = xs[k].reshape(2 * Rs, D)

        def one(j, carry):
            kv[j, k] = mm(rows, wkv[j]).astype(BF).reshape(NC, 2 * RC, W)
            return carry

        lax.fori_loop(2 * layer, 2 * layer + 2, one, 0)

    def project_chunk(k, ch):
        rows = xs[k, ch].reshape(2 * RC, D)

        def one(j, carry):
            kv[j, k, ch] = mm(rows, wkv[j]).astype(BF)
            return carry

        lax.fori_loop(0, 2, one, 0)

    G = max(1, min(S, GROUP_ROWS // H))
    while S % G:
        G -= 1

    def attend(layer, j):
        def group(base):
            blocks = pl.ds(base, G)
            lanes = lax.broadcasted_iota(jnp.int32, (G * H, LANES), 1)
            packed = jnp.zeros((G * H, LANES), F32)
            for h in range(heads):
                cols = slice(h * HD, (h + 1) * HD)
                query = qall[layer, j, blocks, :, cols].reshape(G * H, HD)
                keys = kv[2 * layer, :, :, :, cols].reshape(n * Rs, HD)
                values = kv[2 * layer + 1, :, :, :, cols].reshape(n * Rs, HD)
                scores = (
                    lax.dot_general(
                        query, keys, (((1,), (1,)), ((), ())), preferred_element_type=F32
                    )
                    * scale
                )
                top = jnp.max(scores, axis=-1, keepdims=True)
                raised = jnp.exp(scores - top)
                total = jnp.sum(raised, axis=-1, keepdims=True)
                osend[layer, j, blocks, :, cols] = (
                    mm(raised.astype(BF), values).astype(BF).reshape(G, H, HD)
                )
                packed = jnp.where(lanes == 2 * h, top, packed)
                packed = jnp.where(lanes == 2 * h + 1, total, packed)
            stats = packed.T[: 2 * heads]
            for b in range(G):
                ssend[layer, j, base + b] = jnp.concatenate(
                    [stats[r : r + 1, b * H : (b + 1) * H] for r in range(2 * heads)], axis=1
                )

        if G == S:
            group(0)
        else:

            def one(g, carry):
                group(g * G)
                return carry

            lax.fori_loop(0, S // G, one, 0)
        for block in far_blocks:
            for src, dst, number, sem in (
                (ssend, srecv, 6, s_recv),
                (osend, orecv, 5, r_recv),
            ):
                remote(
                    src.at[layer, j, block],
                    dst.at[layer, j, s],
                    sent.at[number],
                    sem.at[j],
                    "sp",
                    block,
                ).start()
        orecv[layer, j, s] = osend[layer, j, s]
        srecv[layer, j, s] = ssend[layer, j, s]

    def combine(layer, j):
        wait_for(s_recv.at[j], srecv.at[layer, j, most])
        wait_for(r_recv.at[j], orecv.at[layer, j, most])
        rows = [srecv[layer, j, b] for b in range(S)]
        room = -S % LANES
        stats = jnp.concatenate([*rows, jnp.zeros((room, 2 * heads * H), F32)], axis=0).T
        for h in range(heads):
            cols = slice(h * HD, (h + 1) * HD)
            top_rows = stats[2 * h * H : (2 * h + 1) * H]
            total_rows = stats[(2 * h + 1) * H : (2 * h + 2) * H]
            tops = [top_rows[:, b : b + 1] for b in range(S)]
            highest = functools.reduce(jnp.maximum, tops)
            total = jnp.zeros((H, 1), F32)
            summed = jnp.zeros((H, HD), F32)
            for b in range(S):
                factor = jnp.exp(tops[b] - highest)
                total = total + factor * total_rows[:, b : b + 1]
                summed = summed + factor * orecv[layer, j, b, :, cols].astype(F32)
            att[j, :, cols] = (summed / total).astype(BF)
        rows = att[j]
        for ch in range(C):
            cols = slice(ch * (D // C), (ch + 1) * (D // C))
            pf[j, :, :, cols] = mm(rows, wo[layer, :, cols]).reshape(2, Rh, D // C)
            p1s[layer, j, ch] = pf[j, other, :, cols].astype(BF)
            remote(
                p1s.at[layer, j, ch],
                p1r.at[layer, j, ch],
                sent.at[7],
                p1_recv.at[j, ch],
                "tp",
                peer,
            ).start()

    def spread(layer, j):
        for ch in range(C):
            cols = slice(ch * (D // C), (ch + 1) * (D // C))
            wait_for(p1_recv.at[j, ch], p1r.at[layer, j, ch])
            chip_sum = pf[j, c, :, cols] + p1r[layer, j, ch].astype(F32)
            p2s[layer, j, ch] = chip_sum.astype(BF)
            for i in offsets:
                remote(
                    p2s.at[layer, j, ch],
                    p2r.at[layer, j, ch, i - 1],
                    sent.at[8],
                    p2_recv.at[j, ch, i - 1],
                    "tp",
                    to_chip(i) * 2 + c,
                ).start()
            residual[j, :, cols] = residual[j, :, cols] + chip_sum

    def settle(layer, j, gain):
        for ch in range(C):
            cols = slice(ch * (D // C), (ch + 1) * (D // C))
            for i in offsets:
                wait_for(p2_recv.at[j, ch, i - 1], p2r.at[layer, j, ch, i - 1])
                residual[j, :, cols] = residual[j, :, cols] + p2r[layer, j, ch, i - 1].astype(F32)
        xt[layer + 1, j, c] = normed_rows(residual[j], gain).astype(BF)
        share_rows(layer + 1, j, j)

    def turn_weight(src, dst):
        def one(j, carry):
            rows = pl.ds(pl.multiple_of(j * GROUP_ROWS, GROUP_ROWS), GROUP_ROWS)
            dst[rows] = src[:, rows].T
            return carry

        lax.fori_loop(0, D // GROUP_ROWS, one, 0)

    with scope("barrier"):
        pl.semaphore_wait(barrier, X + S - 1)
    load_t.wait()
    for i in offsets:
        remote(
            traw.at[x], traw.at[x], sent.at[0], tr_recv.at[i - 1], "tp", to_chip(i) * 2 + c
        ).start()
    for copy in load_kv[0]:
        copy.start()
    for copy in load_small:
        copy.wait()
    first_rows(x)
    load_s.wait()
    with scope("norm_source"):
        for ch in range(NC):
            rows = sv[ch * RC : (ch + 1) * RC].astype(F32)
            xs[x, ch, c] = normed_rows(rows, source_gain[...]).astype(BF)
            mine = xs.at[x, ch, c]
            for i in offsets:
                remote(
                    mine, mine, sent.at[2], sx_recv.at[ch, i - 1], "tp", to_chip(i) * 2 + c
                ).start()
            remote(mine, mine, sent.at[3], own_recv.at[0], "tp", peer).start()
    with scope("q0own"):
        load_q[0].wait()
        first_queries(x)
    for copy in [*load_kv[1], *load_m, *load_late]:
        copy.start()
    with scope("proj_chip0"):
        wait_for(own_recv.at[0], xs.at[x, :, other])
        for copy in load_kv[0]:
            copy.wait()
        project_chip(0, x)
    with scope("target_far"):
        for i in offsets:
            k = from_chip(i)
            wait_for(tr_recv.at[i - 1], traw.at[k])
            first_rows(k)
    for copy in [load_q[1], *load_o]:
        copy.start()
    with scope("proj_chip1"):
        for copy in load_kv[1]:
            copy.wait()
        project_chip(1, x)
    with scope("q0far"):
        for i in offsets:
            first_queries(from_chip(i))
    turns = [(load_m[0], wg, wgt), (load_m[1], wu, wut)]
    for ch in range(NC):
        if ch and turns:
            with scope("turn"):
                copy, src, dst = turns.pop(0)
                copy.wait()
                turn_weight(src, dst)
        with scope(f"forward{ch}"):
            for i in offsets:
                landed = xs.at[from_chip(i), ch, c]
                wait_for(sx_recv.at[ch, i - 1], landed)
                remote(landed, landed, sent.at[3], sd_recv.at[ch, i - 1], "tp", peer).start()
        with scope(f"proj{ch}"):
            for i in offsets:
                wait_for(sd_recv.at[ch, i - 1], xs.at[from_chip(i), ch, other])
                project_chunk(from_chip(i), ch)
    for k in range(X):
        wait_for(q_recv.at[k], qall.at[0, streams(k), most])
    for j in order:
        with scope(f"attend0{j}"):
            attend(0, j)
    with scope("proj_rest"):
        for i in offsets:
            project_chip(1, from_chip(i))
    for copy in [*load_o, load_q[1], *load_late, load_m[2]]:
        copy.wait()
    for i in range(NS + 2):
        if i < NS:
            with scope(f"combine0{i}"):
                combine(0, order[i])
        if i >= 2:
            with scope(f"query{i - 2}"):
                next_queries(order[i - 2])
        if EARLY and i == NS:
            with scope("attend10"):
                await_queries(order[0])
                attend(1, order[0])
        if i < NS:
            with scope(f"spread0{i}"):
                spread(0, order[i])
        if 1 <= i <= NS:
            with scope(f"settle0{i - 1}"):
                settle(0, order[i - 1], attend_gain[1:2])
    pads = ((gpad, wgt), (upad, wut))

    def halo_out(number):
        return remote(
            hs.at[number],
            hr.at[number],
            sent.at[11 + number],
            h_recv.at[number],
            "sp",
            lax.rem(s + 1, S),
        )

    def lift(k):
        for h in range(SUB):
            await_rows(2, k * SUB + h, k * SUB + h)
        mixed = xt[2, streams(k)].reshape(SUB * H, D)
        for number, (pad, weight) in enumerate(pads):
            lifted = mm(mixed, weight[...]).astype(BF).astype(F32)
            if k == X - 1:
                hs[number] = lifted[SUB * H - 8 :]

                @pl.when(s < S - 1)
                def _():
                    halo_out(number).start()

            for piece in range(2 * SUB):
                part, core = divmod(piece, 2)
                start = 8 + (2 * k + core) * Rt + part * Rh
                pad[start : start + Rh] = lifted[piece * Rh : (piece + 1) * Rh]

    lifts = [*reversed(range(X))]

    def step(name):
        kind, i = name[0], int(name[1:])
        with scope(name):
            if kind == "r":
                relay(order[i])
            elif kind == "a":
                await_queries(order[i])
                attend(1, order[i])
            elif kind == "c":
                combine(1, order[i])
            elif kind == "s":
                spread(1, order[i])
            elif kind == "e":
                settle(1, order[i], mixer_gain[...])
            else:
                lift(lifts[i])

    if NS == 4:
        steps = STEPS
    else:
        steps = [f"r{i}" for i in range(NS)] + [f"a{i}" for i in range(EARLY, NS)]
        steps += [f"{kind}{i}" for i in range(NS) for kind in "cse"]
        steps += [f"l{i}" for i in range(X)]
    for name in steps:
        step(name)

    def hidden_rows(start, stop):
        def convolved(pad, taps):
            return (
                taps[0:1] * pad[6 + start : 6 + stop]
                + taps[1:2] * pad[7 + start : 7 + stop]
                + taps[2:3] * pad[8 + start : 8 + stop]
            )

        gate = convolved(gpad, gate_taps)
        hid[start:stop] = (gate / (1.0 + jnp.exp(-gate)) * convolved(upad, up_taps)).astype(BF)

    with scope("hidden"):
        hidden_rows(16, T)

    @pl.when(s == 0)
    def _():
        for pad, _weight in pads:
            pad[:8] = jnp.zeros((8, F), F32)

    @pl.when(s > 0)
    def _():
        for number, (pad, _weight) in enumerate(pads):
            halo_out(number).wait_recv()
            pad[:8] = hr[number]

    @pl.when(s < S - 1)
    def _():
        for number in range(2):
            halo_out(number).wait_send()

    hidden_rows(0, 16)

    def down_cols(ch):
        return slice(ch * (D // C2), (ch + 1) * (D // C2))

    with scope("down_mm"):
        rows = hid[...]
        for ch in range(C2):
            dpf[:, :, :, down_cols(ch)] = mm(rows, wd[:, down_cols(ch)]).reshape(
                X, 2, Rt, D // C2
            )
            d1s[ch] = dpf[:, other, :, down_cols(ch)].astype(BF)
            remote(d1s.at[ch], d1r.at[ch], sent.at[9], d1_recv.at[ch], "tp", peer).start()
    own = streams(x)
    with scope("down_pair"):
        for ch in range(C2):
            cols = down_cols(ch)
            wait_for(d1_recv.at[ch], d1r.at[ch])
            for i in offsets:
                k = to_chip(i)
                d2s[ch, i - 1] = (dpf[k, c, :, cols] + d1r[ch, k].astype(F32)).astype(BF)
                remote(
                    d2s.at[ch, i - 1],
                    d2r.at[ch, i - 1],
                    sent.at[10],
                    d2_recv.at[ch, i - 1],
                    "tp",
                    k * 2 + c,
                ).start()
            added = dpf[x, c, :, cols] + d1r[ch, x].astype(F32)
            residual[own, :, cols] = residual[own, :, cols] + added.reshape(SUB, Rh, D // C2)
    with scope("drain"):
        first = pl.ds(0, X - 1)
        wait_sent(0, traw.at[first])
        wait_sent(1, xt.at[:, :, 0])
        wait_sent(2, xs.at[first, :, 0])
        wait_sent(3, xs.at[:, :, 0])
        wait_sent(4, qall.at[:, :, most])
        wait_sent(5, osend.at[:, :, most])
        wait_sent(6, ssend.at[:, :, most])
        wait_sent(7, p1s)
        wait_sent(8, p2r)
        wait_sent(9, d1s)
    with scope("down_far"):
        for ch in range(C2):
            cols = down_cols(ch)
            for i in offsets:
                wait_for(d2_recv.at[ch, i - 1], d2r.at[ch, i - 1])
                added = d2r[ch, i - 1].astype(F32)
                residual[own, :, cols] = residual[own, :, cols] + added.reshape(SUB, Rh, D // C2)
    result[...] = normed_rows(residual[own].reshape(Rt, D), final_gain[...]).astype(BF)
    wait_sent(10, d2s)


def body(n, S, *arrays):
    (
        source,
        target,
        source_gain,
        attend_gain,
        query_weight,
        key_weight,
        value_weight,
        out_weight,
        mixer_gain,
        gate_weight,
        up_weight,
        gate_taps,
        up_taps,
        down_weight,
        final_gain,
    ) = arrays
    Rs, D = source.shape
    Rt = target.shape[0]
    W = query_weight.shape[2]
    F = gate_weight.shape[1]
    T = n * Rt
    X = n // 2
    SUB = STREAMS_PER_CHIP
    NS = SUB * X
    Rh = Rt // SUB
    H = 2 * Rh
    NC = SOURCE_CHUNKS
    C = OUT_CHUNKS
    C2 = DOWN_CHUNKS
    RC = Rs // NC
    hbm = pl.BlockSpec(memory_space=pl.ANY)
    dma = pltpu.SemaphoreType.DMA
    scratch = [
        pltpu.VMEM((1, D), F32),
        pltpu.VMEM((2, D), F32),
        pltpu.VMEM((1, D), F32),
        pltpu.VMEM((1, D), F32),
        pltpu.VMEM((3, F), F32),
        pltpu.VMEM((3, F), F32),
        pltpu.VMEM((Rs, D), BF),
        pltpu.VMEM((X, Rt, D), BF),
        pltpu.VMEM((2, D, W), BF),
        pltpu.VMEM((4, D, W), BF),
        pltpu.VMEM((2, W, D), BF),
        pltpu.VMEM((F, D), BF),
        pltpu.VMEM((F, D), BF),
        pltpu.VMEM((D, F), BF),
        pltpu.VMEM((D, F), BF),
        pltpu.VMEM((F, D), BF),
        pltpu.VMEM((X, NC, 2, RC, D), BF),
        pltpu.VMEM((3, NS, 2, Rh, D), BF),
        pltpu.VMEM((4, X, NC, 2 * RC, W), BF),
        pltpu.VMEM((2, NS, S, H, W), BF),
        pltpu.VMEM((2, NS, S, H, W), BF),
        pltpu.VMEM((2, NS, S, H, W), BF),
        pltpu.VMEM((2, NS, S, 1, 2 * (W // HD) * H), F32),
        pltpu.VMEM((2, NS, S, 1, 2 * (W // HD) * H), F32),
        pltpu.VMEM((NS, 2, Rh, D), F32),
        pltpu.VMEM((NS, H, W), BF),
        pltpu.VMEM((2, NS, C, Rh, D // C), BF),
        pltpu.VMEM((2, NS, C, Rh, D // C), BF),
        pltpu.VMEM((2, NS, C, Rh, D // C), BF),
        pltpu.VMEM((2, NS, C, X - 1, Rh, D // C), BF),
        pltpu.VMEM((X, 2, Rt, D), F32),
        pltpu.VMEM((C2, X, Rt, D // C2), BF),
        pltpu.VMEM((C2, X, Rt, D // C2), BF),
        pltpu.VMEM((C2, X - 1, Rt, D // C2), BF),
        pltpu.VMEM((C2, X - 1, Rt, D // C2), BF),
        pltpu.VMEM((2, 8, F), F32),
        pltpu.VMEM((2, 8, F), F32),
        pltpu.VMEM((T + 8, F), F32),
        pltpu.VMEM((T + 8, F), F32),
        pltpu.VMEM((T, F), BF),
        pltpu.VMEM((NS, Rh, D), F32),
        dma((12,)),
        dma((13,)),
        dma((X - 1,)),
        dma((NS,)),
        dma((NC, X - 1)),
        dma((NC, X - 1)),
        dma((1,)),
        dma((NS,)),
        dma((NS,)),
        dma((NS,)),
        dma((NS,)),
        dma((NS, C)),
        dma((NS, C, X - 1)),
        dma((C2,)),
        dma((C2, X - 1)),
        dma((2,)),
    ]
    return pl.pallas_call(
        functools.partial(kernel, n, S),
        out_shape=pltpu.VMEM((Rt, D), BF),
        in_specs=[hbm] * 15,
        out_specs=pl.BlockSpec(memory_space=pltpu.VMEM),
        scratch_shapes=scratch,
        compiler_params=pltpu.CompilerParams(
            collective_id=0, has_side_effects=True, vmem_limit_bytes=66000000
        ),
    )(
        source,
        target,
        source_gain.reshape(1, D),
        attend_gain,
        query_weight,
        key_weight,
        value_weight,
        out_weight,
        mixer_gain.reshape(1, D),
        gate_weight.T,
        up_weight.T,
        gate_taps,
        up_taps,
        down_weight,
        final_gain.reshape(1, D),
    )


def solution(mesh):
    placed = (
        P(("grp", "sp", "tp"), None),
        P(("grp", "sp", "tp"), None),
        P(),
        P(),
        P(None, None, "tp"),
        P(None, None, "tp"),
        P(None, None, "tp"),
        P(None, "tp", None),
        P(),
        P(None, "tp"),
        P(None, "tp"),
        P(None, "tp"),
        P(None, "tp"),
        P("tp", None),
        P(),
    )
    return jax.shard_map(
        functools.partial(body, mesh.shape["tp"], mesh.shape["sp"]),
        mesh=mesh,
        in_specs=placed,
        out_specs=P(("grp", "sp", "tp"), None),
        check_vma=False,
    )
```

```python
import functools

import jax
import jax.numpy as jnp
from jax import lax
from jax.experimental import pallas as pl
from jax.experimental.pallas import tpu as pltpu
from jax.sharding import PartitionSpec as P

HD = 256
EPS = 1e-06
LANES = 128
SOURCE_CHUNKS = 4
STREAMS_PER_CHIP = 2
RELAYED = (1, 2)
STEPS = (
    "r1",
    "a0",
    "r2",
    "a1",
    "c0",
    "a2",
    "s0",
    "a3",
    "c1",
    "s1",
    "e0",
    "c2",
    "s2",
    "e1",
    "c3",
    "s3",
    "l0",
    "e2",
    "e3",
    "l1",
)
OUT_CHUNKS = 2
DOWN_CHUNKS = 4
RAW = 1
DOWN_RAW = 1
GROUP_ROWS = 256
MESH = pl.DeviceIdType.MESH
BF = jnp.bfloat16
F32 = jnp.float32


def normed_rows(wide, gain):
    return wide * lax.rsqrt(jnp.mean(wide * wide, axis=-1, keepdims=True) + EPS) * gain


def mm(a, b):
    return jnp.dot(a, b, preferred_element_type=F32)


def scope(name):
    return jax.named_scope(name)


def kernel(
    n,
    S,
    source,
    target,
    source_gain_in,
    attend_gain_in,
    query_weight,
    key_weight,
    value_weight,
    out_weight,
    mixer_gain_in,
    gate_weight,
    up_weight,
    gate_taps_in,
    up_taps_in,
    down_weight,
    final_gain_in,
    result,
    source_gain,
    attend_gain,
    mixer_gain,
    final_gain,
    gate_taps,
    up_taps,
    sv,
    traw,
    wq,
    wkv,
    wo,
    wg,
    wu,
    wgt,
    wut,
    wd,
    xs,
    xt,
    kv,
    qall,
    osend,
    orecv,
    ssend,
    srecv,
    pf,
    att,
    p1s,
    p1r,
    p2s,
    p2r,
    rr,
    dpf,
    d1s,
    d1r,
    d2s,
    d2r,
    rd,
    hs,
    hr,
    gpad,
    upad,
    hid,
    residual,
    load_sem,
    sent,
    tr_recv,
    n_recv,
    sx_recv,
    sd_recv,
    own_recv,
    q_recv,
    cross_recv,
    r_recv,
    s_recv,
    p1_recv,
    p2_recv,
    rr_recv,
    d1_recv,
    d2_recv,
    rd_recv,
    h_recv,
):
    X = n // 2
    Rs, D = source.shape
    Rt = target.shape[0]
    W = wq.shape[2]
    T = n * Rt
    NS, Rh = residual.shape[:2]
    SUB = NS // X
    H = 2 * Rh
    heads = W // HD
    F = wg.shape[0]
    NC = xs.shape[1]
    RC = Rs // NC
    C = p1s.shape[2]
    C2 = d1s.shape[0]
    scale = HD ** (-0.5)
    t = lax.axis_index("tp")
    s = lax.axis_index("sp")
    x = lax.div(t, 2)
    c = lax.rem(t, 2)
    other = 1 - c
    peer = x * 2 + other
    offsets = range(1, X)
    order = [k * SUB + h for k in reversed(range(X)) for h in range(SUB)]

    def to_chip(i):
        return lax.rem(x + i, X)

    def from_chip(i):
        return lax.rem(x + X - i, X)

    def streams(k):
        return pl.ds(k * SUB, SUB)

    def remote(src, dst, ss, rs, axis, where):
        return pltpu.make_async_remote_copy(
            src_ref=src,
            dst_ref=dst,
            send_sem=ss,
            recv_sem=rs,
            device_id={axis: where},
            device_id_type=MESH,
        )

    def wait_for(sem, ref):
        remote(ref, ref, sent.at[0], sem, "tp", peer).wait_recv()

    def wait_sent(number, ref):
        remote(ref, ref, sent.at[number], own_recv.at[0], "tp", peer).wait_send()

    far_blocks = []
    low = s * 0
    high = low + (S - 1)
    for _ in range(S - 1):
        left = lax.div(2 * s - low - high + S, S)
        far_blocks.append(left * low + (1 - left) * high)
        low = low + left
        high = high - (1 - left)
    most = pl.ds(0, S - 1)
    half = S // 2
    RELAY = S % 2 == 0 and S > 2

    barrier = pltpu.get_barrier_semaphore()
    pl.semaphore_signal(barrier, inc=1, device_id={"tp": peer}, device_id_type=MESH)
    for i in offsets:
        pl.semaphore_signal(
            barrier, inc=1, device_id={"tp": to_chip(i) * 2 + c}, device_id_type=MESH
        )
        pl.semaphore_signal(
            barrier, inc=1, device_id={"tp": to_chip(i) * 2 + other}, device_id_type=MESH
        )
    for block in far_blocks:
        pl.semaphore_signal(barrier, inc=1, device_id={"sp": block}, device_id_type=MESH)

    def load(number, src, dst):
        return pltpu.make_async_copy(src, dst, load_sem.at[number])

    load_t = load(0, target, traw.at[x])
    load_s = load(1, source, sv)
    load_small = [load(2, attend_gain_in, attend_gain), load(3, source_gain_in, source_gain)]
    load_late = [
        load(0, mixer_gain_in, mixer_gain),
        load(1, final_gain_in, final_gain),
        load(2, gate_taps_in, gate_taps),
        load(3, up_taps_in, up_taps),
    ]
    load_q = [load(4, query_weight.at[l], wq.at[l]) for l in range(2)]
    load_kv = [
        [
            load(5 + 2 * l, key_weight.at[l], wkv.at[2 * l]),
            load(6 + 2 * l, value_weight.at[l], wkv.at[2 * l + 1]),
        ]
        for l in range(2)
    ]
    load_o = [load(5 + l, out_weight.at[l], wo.at[l]) for l in range(2)]
    load_m = [load(9, gate_weight, wg), load(10, up_weight, wu), load(11, down_weight, wd)]
    for copy in [load_t, *load_small, load_s, load_q[0]]:
        copy.start()

    def share_rows(a, rows, number):
        remote(
            xt.at[a, rows, c], xt.at[a, rows, c], sent.at[1], n_recv.at[number], "tp", peer
        ).start()

    def await_rows(a, rows, number):
        wait_for(n_recv.at[number], xt.at[a, rows, other])

    def first_rows(k):
        rows = traw[k].astype(F32)
        residual[streams(k)] = rows.reshape(SUB, Rh, D)
        xt[0, streams(k), c] = normed_rows(rows, attend_gain[0:1]).astype(BF).reshape(SUB, Rh, D)
        share_rows(0, streams(k), k)

    def first_queries(k):
        await_rows(0, streams(k), k)
        rows = xt[0, streams(k)].reshape(SUB * H, D)
        qall[0, streams(k), s] = mm(rows, wq[0]).astype(BF).reshape(SUB, H, W)
        for block in far_blocks:
            mine = qall.at[0, streams(k), s]
            remote(mine, mine, sent.at[4], q_recv.at[k], "sp", block).start()

    def next_queries(j):
        await_rows(1, j, j)
        qall[1, j, s] = mm(xt[1, j].reshape(H, D), wq[1]).astype(BF)
        if relayed(j):
            mine = qall.at[1, j, s]
            remote(mine, mine, sent.at[4], cross_recv.at[j], "sp", lax.rem(s + half, S)).start()
            to_mates(j, s)
        else:
            for block in far_blocks:
                mine = qall.at[1, j, s]
                remote(mine, mine, sent.at[4], q_recv.at[j], "sp", block).start()

    def to_mates(j, block):
        for m in range(1, half):
            mate = lax.div(s, half) * half + lax.rem(s + m, half)
            rows = qall.at[1, j, block]
            remote(rows, rows, sent.at[4], q_recv.at[j], "sp", mate).start()

    def relayed(j):
        return RELAY and order.index(j) in RELAYED

    def relay(j):
        if relayed(j):
            block = lax.rem(s + half, S)
            wait_for(cross_recv.at[j], qall.at[1, j, block])
            to_mates(j, block)

    def await_queries(j):
        count = 2 * (half - 1) if relayed(j) else S - 1
        wait_for(q_recv.at[j], qall.at[1, j, pl.ds(0, count)])

    def project_chip(layer, k):
        rows = xs[k].reshape(2 * Rs, D)

        def one(j, carry):
            kv[j, k] = mm(rows, wkv[j]).astype(BF).reshape(NC, 2 * RC, W)
            return carry

        lax.fori_loop(2 * layer, 2 * layer + 2, one, 0)

    def project_chunk(k, ch):
        rows = xs[k, ch].reshape(2 * RC, D)

        def one(j, carry):
            kv[j, k, ch] = mm(rows, wkv[j]).astype(BF)
            return carry

        lax.fori_loop(0, 2, one, 0)

    G = max(1, min(S, GROUP_ROWS // H))
    while S % G:
        G -= 1

    def attend(layer, j):
        def group(base):
            blocks = pl.ds(base, G)
            lanes = lax.broadcasted_iota(jnp.int32, (G * H, LANES), 1)
            packed = jnp.zeros((G * H, LANES), F32)
            for h in range(heads):
                cols = slice(h * HD, (h + 1) * HD)
                query = qall[layer, j, blocks, :, cols].reshape(G * H, HD)
                keys = kv[2 * layer, :, :, :, cols].reshape(n * Rs, HD)
                values = kv[2 * layer + 1, :, :, :, cols].reshape(n * Rs, HD)
                scores = (
                    lax.dot_general(
                        query, keys, (((1,), (1,)), ((), ())), preferred_element_type=F32
                    )
                    * scale
                )
                top = jnp.max(scores, axis=-1, keepdims=True)
                raised = jnp.exp(scores - top)
                total = jnp.sum(raised, axis=-1, keepdims=True)
                osend[layer, j, blocks, :, cols] = (
                    mm(raised.astype(BF), values).astype(BF).reshape(G, H, HD)
                )
                packed = jnp.where(lanes == 2 * h, top, packed)
                packed = jnp.where(lanes == 2 * h + 1, total, packed)
            stats = packed.T[: 2 * heads]
            for b in range(G):
                ssend[layer, j, base + b] = jnp.concatenate(
                    [stats[r : r + 1, b * H : (b + 1) * H] for r in range(2 * heads)], axis=1
                )

        if G == S:
            group(0)
        else:

            def one(g, carry):
                group(g * G)
                return carry

            lax.fori_loop(0, S // G, one, 0)
        for block in far_blocks:
            for src, dst, number, sem in (
                (ssend, srecv, 6, s_recv),
                (osend, orecv, 5, r_recv),
            ):
                remote(
                    src.at[layer, j, block],
                    dst.at[layer, j, s],
                    sent.at[number],
                    sem.at[j],
                    "sp",
                    block,
                ).start()
        orecv[layer, j, s] = osend[layer, j, s]
        srecv[layer, j, s] = ssend[layer, j, s]

    def combine(layer, j):
        wait_for(s_recv.at[j], srecv.at[layer, j, most])
        wait_for(r_recv.at[j], orecv.at[layer, j, most])
        rows = [srecv[layer, j, b] for b in range(S)]
        room = -S % LANES
        stats = jnp.concatenate([*rows, jnp.zeros((room, 2 * heads * H), F32)], axis=0).T
        for h in range(heads):
            cols = slice(h * HD, (h + 1) * HD)
            top_rows = stats[2 * h * H : (2 * h + 1) * H]
            total_rows = stats[(2 * h + 1) * H : (2 * h + 2) * H]
            tops = [top_rows[:, b : b + 1] for b in range(S)]
            highest = functools.reduce(jnp.maximum, tops)
            total = jnp.zeros((H, 1), F32)
            summed = jnp.zeros((H, HD), F32)
            for b in range(S):
                factor = jnp.exp(tops[b] - highest)
                total = total + factor * total_rows[:, b : b + 1]
                summed = summed + factor * orecv[layer, j, b, :, cols].astype(F32)
            att[j, :, cols] = (summed / total).astype(BF)
        rows = att[j]
        for ch in range(C):
            cols = slice(ch * (D // C), (ch + 1) * (D // C))
            pf[j, :, :, cols] = mm(rows, wo[layer, :, cols]).reshape(2, Rh, D // C)
            p1s[layer, j, ch] = pf[j, other, :, cols].astype(BF)
            remote(
                p1s.at[layer, j, ch],
                p1r.at[layer, j, ch],
                sent.at[7],
                p1_recv.at[j, ch],
                "tp",
                peer,
            ).start()
            if ch < RAW:
                p2s[layer, j, ch] = pf[j, c, :, cols].astype(BF)
                for i in offsets:
                    chip_copy(layer, j, ch, i).start()
                    remote(
                        p1s.at[layer, j, ch],
                        rr.at[layer, j, ch, i - 1],
                        sent.at[13],
                        rr_recv.at[j, ch, i - 1],
                        "tp",
                        to_chip(i) * 2 + other,
                    ).start()

    def chip_copy(layer, j, ch, i):
        return remote(
            p2s.at[layer, j, ch],
            p2r.at[layer, j, ch, i - 1],
            sent.at[8],
            p2_recv.at[j, ch, i - 1],
            "tp",
            to_chip(i) * 2 + c,
        )

    def spread(layer, j):
        for ch in range(C):
            cols = slice(ch * (D // C), (ch + 1) * (D // C))
            wait_for(p1_recv.at[j, ch], p1r.at[layer, j, ch])
            chip_sum = pf[j, c, :, cols] + p1r[layer, j, ch].astype(F32)
            if ch >= RAW:
                p2s[layer, j, ch] = chip_sum.astype(BF)
                for i in offsets:
                    chip_copy(layer, j, ch, i).start()
            residual[j, :, cols] = residual[j, :, cols] + chip_sum

    def settle(layer, j, gain):
        for ch in range(C):
            cols = slice(ch * (D // C), (ch + 1) * (D // C))
            for i in offsets:
                wait_for(p2_recv.at[j, ch, i - 1], p2r.at[layer, j, ch, i - 1])
                residual[j, :, cols] = residual[j, :, cols] + p2r[layer, j, ch, i - 1].astype(F32)
                if ch < RAW:
                    wait_for(rr_recv.at[j, ch, i - 1], rr.at[layer, j, ch, i - 1])
                    residual[j, :, cols] = residual[j, :, cols] + rr[
                        layer, j, ch, i - 1
                    ].astype(F32)
        xt[layer + 1, j, c] = normed_rows(residual[j], gain).astype(BF)
        share_rows(layer + 1, j, j)

    def turn_weight(src, dst):
        def one(j, carry):
            rows = pl.ds(pl.multiple_of(j * GROUP_ROWS, GROUP_ROWS), GROUP_ROWS)
            dst[rows] = src[:, rows].T
            return carry

        lax.fori_loop(0, D // GROUP_ROWS, one, 0)

    with scope("barrier"):
        pl.semaphore_wait(barrier, 2 * X - 1 + S - 1)
    load_t.wait()
    for i in offsets:
        remote(
            traw.at[x], traw.at[x], sent.at[0], tr_recv.at[i - 1], "tp", to_chip(i) * 2 + c
        ).start()
    for copy in load_kv[0]:
        copy.start()
    for copy in load_small:
        copy.wait()
    first_rows(x)
    load_s.wait()
    with scope("norm_source"):
        for ch in range(NC):
            rows = sv[ch * RC : (ch + 1) * RC].astype(F32)
            xs[x, ch, c] = normed_rows(rows, source_gain[...]).astype(BF)
            mine = xs.at[x, ch, c]
            for i in offsets:
                remote(
                    mine, mine, sent.at[2], sx_recv.at[ch, i - 1], "tp", to_chip(i) * 2 + c
                ).start()
            remote(mine, mine, sent.at[3], own_recv.at[0], "tp", peer).start()
    with scope("q0own"):
        load_q[0].wait()
        first_queries(x)
    for copy in [*load_kv[1], *load_m, *load_late]:
        copy.start()
    with scope("proj_chip0"):
        wait_for(own_recv.at[0], xs.at[x, :, other])
        for copy in load_kv[0]:
            copy.wait()
        project_chip(0, x)
    with scope("target_far"):
        for i in offsets:
            k = from_chip(i)
            wait_for(tr_recv.at[i - 1], traw.at[k])
            first_rows(k)
    for copy in [load_q[1], *load_o]:
        copy.start()
    with scope("proj_chip1"):
        for copy in load_kv[1]:
            copy.wait()
        project_chip(1, x)
    with scope("q0far"):
        for i in offsets:
            first_queries(from_chip(i))
    turns = [(load_m[0], wg, wgt), (load_m[1], wu, wut)]
    for ch in range(NC):
        if ch and turns:
            with scope("turn"):
                copy, src, dst = turns.pop(0)
                copy.wait()
                turn_weight(src, dst)
        with scope(f"forward{ch}"):
            for i in offsets:
                landed = xs.at[from_chip(i), ch, c]
                wait_for(sx_recv.at[ch, i - 1], landed)
                remote(landed, landed, sent.at[3], sd_recv.at[ch, i - 1], "tp", peer).start()
        with scope(f"proj{ch}"):
            for i in offsets:
                wait_for(sd_recv.at[ch, i - 1], xs.at[from_chip(i), ch, other])
                project_chunk(from_chip(i), ch)
    for k in range(X):
        wait_for(q_recv.at[k], qall.at[0, streams(k), most])
    for j in order:
        with scope(f"attend0{j}"):
            attend(0, j)
    with scope("proj_rest"):
        for i in offsets:
            project_chip(1, from_chip(i))
    for copy in [*load_o, load_q[1], *load_late, load_m[2]]:
        copy.wait()
    for i in range(NS + 2):
        if i < NS:
            with scope(f"combine0{i}"):
                combine(0, order[i])
        if i >= 2:
            with scope(f"query{i - 2}"):
                next_queries(order[i - 2])
        if i < NS:
            with scope(f"spread0{i}"):
                spread(0, order[i])
        if 1 <= i <= NS:
            with scope(f"settle0{i - 1}"):
                settle(0, order[i - 1], attend_gain[1:2])
    pads = ((gpad, wgt), (upad, wut))

    def halo_out(number):
        return remote(
            hs.at[number],
            hr.at[number],
            sent.at[11 + number],
            h_recv.at[number],
            "sp",
            lax.rem(s + 1, S),
        )

    def lift(k):
        for h in range(SUB):
            await_rows(2, k * SUB + h, k * SUB + h)
        mixed = xt[2, streams(k)].reshape(SUB * H, D)
        for number, (pad, weight) in enumerate(pads):
            lifted = mm(mixed, weight[...]).astype(BF).astype(F32)
            if k == X - 1:
                hs[number] = lifted[SUB * H - 8 :]

                @pl.when(s < S - 1)
                def _():
                    halo_out(number).start()

            for piece in range(2 * SUB):
                part, core = divmod(piece, 2)
                start = 8 + (2 * k + core) * Rt + part * Rh
                pad[start : start + Rh] = lifted[piece * Rh : (piece + 1) * Rh]

    lifts = [*reversed(range(X))]

    def step(name):
        kind, i = name[0], int(name[1:])
        with scope(name):
            if kind == "r":
                relay(order[i])
            elif kind == "a":
                await_queries(order[i])
                attend(1, order[i])
            elif kind == "c":
                combine(1, order[i])
            elif kind == "s":
                spread(1, order[i])
            elif kind == "e":
                settle(1, order[i], mixer_gain[...])
            else:
                lift(lifts[i])

    if NS == 4:
        steps = STEPS
    else:
        steps = [f"r{i}" for i in range(NS)] + [f"a{i}" for i in range(NS)]
        steps += [f"{kind}{i}" for i in range(NS) for kind in "cse"]
        steps += [f"l{i}" for i in range(X)]
    for name in steps:
        step(name)

    def hidden_rows(start, stop):
        def convolved(pad, taps):
            return (
                taps[0:1] * pad[6 + start : 6 + stop]
                + taps[1:2] * pad[7 + start : 7 + stop]
                + taps[2:3] * pad[8 + start : 8 + stop]
            )

        gate = convolved(gpad, gate_taps)
        hid[start:stop] = (gate / (1.0 + jnp.exp(-gate)) * convolved(upad, up_taps)).astype(BF)

    with scope("hidden"):
        hidden_rows(16, T)

    @pl.when(s == 0)
    def _():
        for pad, _weight in pads:
            pad[:8] = jnp.zeros((8, F), F32)

    @pl.when(s > 0)
    def _():
        for number, (pad, _weight) in enumerate(pads):
            halo_out(number).wait_recv()
            pad[:8] = hr[number]

    @pl.when(s < S - 1)
    def _():
        for number in range(2):
            halo_out(number).wait_send()

    hidden_rows(0, 16)

    def down_cols(ch):
        return slice(ch * (D // C2), (ch + 1) * (D // C2))

    def down_chip(ch, i):
        return remote(
            d2s.at[ch, i - 1],
            d2r.at[ch, i - 1],
            sent.at[10],
            d2_recv.at[ch, i - 1],
            "tp",
            to_chip(i) * 2 + c,
        )

    with scope("down_mm"):
        rows = hid[...]
        for ch in range(C2):
            dpf[:, :, :, down_cols(ch)] = mm(rows, wd[:, down_cols(ch)]).reshape(
                X, 2, Rt, D // C2
            )
            d1s[ch] = dpf[:, other, :, down_cols(ch)].astype(BF)
            remote(d1s.at[ch], d1r.at[ch], sent.at[9], d1_recv.at[ch], "tp", peer).start()
            if ch < DOWN_RAW:
                for i in offsets:
                    k = to_chip(i)
                    d2s[ch, i - 1] = dpf[k, c, :, down_cols(ch)].astype(BF)
                    down_chip(ch, i).start()
                    remote(
                        d1s.at[ch, k],
                        rd.at[ch, i - 1],
                        sent.at[14],
                        rd_recv.at[ch, i - 1],
                        "tp",
                        k * 2 + other,
                    ).start()
    own = streams(x)
    with scope("down_pair"):
        for ch in range(C2):
            cols = down_cols(ch)
            wait_for(d1_recv.at[ch], d1r.at[ch])
            for i in offsets:
                k = to_chip(i)
                if ch >= DOWN_RAW:
                    d2s[ch, i - 1] = (dpf[k, c, :, cols] + d1r[ch, k].astype(F32)).astype(BF)
                    down_chip(ch, i).start()
            added = dpf[x, c, :, cols] + d1r[ch, x].astype(F32)
            residual[own, :, cols] = residual[own, :, cols] + added.reshape(SUB, Rh, D // C2)
    with scope("drain"):
        first = pl.ds(0, X - 1)
        wait_sent(0, traw.at[first])
        wait_sent(1, xt.at[:, :, 0])
        wait_sent(2, xs.at[first, :, 0])
        wait_sent(3, xs.at[:, :, 0])
        wait_sent(4, qall.at[:, :, most])
        wait_sent(5, osend.at[:, :, most])
        wait_sent(6, ssend.at[:, :, most])
        wait_sent(7, p1s)
        wait_sent(8, p2r)
        wait_sent(9, d1s)
        wait_sent(13, rr)
    with scope("down_far"):
        for ch in range(C2):
            cols = down_cols(ch)
            for i in offsets:
                wait_for(d2_recv.at[ch, i - 1], d2r.at[ch, i - 1])
                added = d2r[ch, i - 1].astype(F32)
                if ch < DOWN_RAW:
                    wait_for(rd_recv.at[ch, i - 1], rd.at[ch, i - 1])
                    added = added + rd[ch, i - 1].astype(F32)
                residual[own, :, cols] = residual[own, :, cols] + added.reshape(SUB, Rh, D // C2)
    result[...] = normed_rows(residual[own].reshape(Rt, D), final_gain[...]).astype(BF)
    wait_sent(10, d2s)
    wait_sent(14, rd)


def body(n, S, *arrays):
    (
        source,
        target,
        source_gain,
        attend_gain,
        query_weight,
        key_weight,
        value_weight,
        out_weight,
        mixer_gain,
        gate_weight,
        up_weight,
        gate_taps,
        up_taps,
        down_weight,
        final_gain,
    ) = arrays
    Rs, D = source.shape
    Rt = target.shape[0]
    W = query_weight.shape[2]
    F = gate_weight.shape[1]
    T = n * Rt
    X = n // 2
    SUB = STREAMS_PER_CHIP
    NS = SUB * X
    Rh = Rt // SUB
    H = 2 * Rh
    NC = SOURCE_CHUNKS
    C = OUT_CHUNKS
    C2 = DOWN_CHUNKS
    RC = Rs // NC
    hbm = pl.BlockSpec(memory_space=pl.ANY)
    dma = pltpu.SemaphoreType.DMA
    scratch = [
        pltpu.VMEM((1, D), F32),
        pltpu.VMEM((2, D), F32),
        pltpu.VMEM((1, D), F32),
        pltpu.VMEM((1, D), F32),
        pltpu.VMEM((3, F), F32),
        pltpu.VMEM((3, F), F32),
        pltpu.VMEM((Rs, D), BF),
        pltpu.VMEM((X, Rt, D), BF),
        pltpu.VMEM((2, D, W), BF),
        pltpu.VMEM((4, D, W), BF),
        pltpu.VMEM((2, W, D), BF),
        pltpu.VMEM((F, D), BF),
        pltpu.VMEM((F, D), BF),
        pltpu.VMEM((D, F), BF),
        pltpu.VMEM((D, F), BF),
        pltpu.VMEM((F, D), BF),
        pltpu.VMEM((X, NC, 2, RC, D), BF),
        pltpu.VMEM((3, NS, 2, Rh, D), BF),
        pltpu.VMEM((4, X, NC, 2 * RC, W), BF),
        pltpu.VMEM((2, NS, S, H, W), BF),
        pltpu.VMEM((2, NS, S, H, W), BF),
        pltpu.VMEM((2, NS, S, H, W), BF),
        pltpu.VMEM((2, NS, S, 1, 2 * (W // HD) * H), F32),
        pltpu.VMEM((2, NS, S, 1, 2 * (W // HD) * H), F32),
        pltpu.VMEM((NS, 2, Rh, D), F32),
        pltpu.VMEM((NS, H, W), BF),
        pltpu.VMEM((2, NS, C, Rh, D // C), BF),
        pltpu.VMEM((2, NS, C, Rh, D // C), BF),
        pltpu.VMEM((2, NS, C, Rh, D // C), BF),
        pltpu.VMEM((2, NS, C, X - 1, Rh, D // C), BF),
        pltpu.VMEM((2, NS, RAW, X - 1, Rh, D // C), BF),
        pltpu.VMEM((X, 2, Rt, D), F32),
        pltpu.VMEM((C2, X, Rt, D // C2), BF),
        pltpu.VMEM((C2, X, Rt, D // C2), BF),
        pltpu.VMEM((C2, X - 1, Rt, D // C2), BF),
        pltpu.VMEM((C2, X - 1, Rt, D // C2), BF),
        pltpu.VMEM((DOWN_RAW, X - 1, Rt, D // C2), BF),
        pltpu.VMEM((2, 8, F), F32),
        pltpu.VMEM((2, 8, F), F32),
        pltpu.VMEM((T + 8, F), F32),
        pltpu.VMEM((T + 8, F), F32),
        pltpu.VMEM((T, F), BF),
        pltpu.VMEM((NS, Rh, D), F32),
        dma((12,)),
        dma((15,)),
        dma((X - 1,)),
        dma((NS,)),
        dma((NC, X - 1)),
        dma((NC, X - 1)),
        dma((1,)),
        dma((NS,)),
        dma((NS,)),
        dma((NS,)),
        dma((NS,)),
        dma((NS, C)),
        dma((NS, C, X - 1)),
        dma((NS, RAW, X - 1)),
        dma((C2,)),
        dma((C2, X - 1)),
        dma((DOWN_RAW, X - 1)),
        dma((2,)),
    ]
    return pl.pallas_call(
        functools.partial(kernel, n, S),
        out_shape=pltpu.VMEM((Rt, D), BF),
        in_specs=[hbm] * 15,
        out_specs=pl.BlockSpec(memory_space=pltpu.VMEM),
        scratch_shapes=scratch,
        compiler_params=pltpu.CompilerParams(
            collective_id=0, has_side_effects=True, vmem_limit_bytes=66000000
        ),
    )(
        source,
        target,
        source_gain.reshape(1, D),
        attend_gain,
        query_weight,
        key_weight,
        value_weight,
        out_weight,
        mixer_gain.reshape(1, D),
        gate_weight.T,
        up_weight.T,
        gate_taps,
        up_taps,
        down_weight,
        final_gain.reshape(1, D),
    )


def solution(mesh):
    placed = (
        P(("grp", "sp", "tp"), None),
        P(("grp", "sp", "tp"), None),
        P(),
        P(),
        P(None, None, "tp"),
        P(None, None, "tp"),
        P(None, None, "tp"),
        P(None, "tp", None),
        P(),
        P(None, "tp"),
        P(None, "tp"),
        P(None, "tp"),
        P(None, "tp"),
        P("tp", None),
        P(),
    )
    return jax.shard_map(
        functools.partial(body, mesh.shape["tp"], mesh.shape["sp"]),
        mesh=mesh,
        in_specs=placed,
        out_specs=P(("grp", "sp", "tp"), None),
        check_vma=False,
    )
```
